32 devices in a mesh: sp: 16 (over z, y, x), tp: 2 (over core).
Axes of the slice: x: 2, y: 2, z: 4, core: 2. Of those that a mesh axis runs over, the one named last changes fastest.
Arguments:
- query_one: bfloat16 [2048, 1024], P('sp', 'tp'), may hold values from -85 to 85
- key_one: bfloat16 [2048, 1024], P('sp', 'tp'), may hold values from -6.5 to 6.5
- query_two: bfloat16 [2048, 1024], P('sp', 'tp'), may hold values from -85 to 85
- key_two: bfloat16 [2048, 1024], P('sp', 'tp'), may hold values from -6.5 to 6.5
- values: bfloat16 [2048, 2048], P('sp', 'tp'), may hold values from -6 to 6
- mix_weight: float32 [8], P('tp'), may hold values from 0.3 to 0.8
- head_gain: float32 [256], replicated, may hold values from 0.1 to 1.9
- residual: bfloat16 [2048, 2048], P(('sp', 'tp')), may hold values from -6 to 6
- out_weight: bfloat16 [2048, 2048], P('tp'), may hold values from -0.125 to 0.125
- norm_gain: float32 [2048], replicated, may hold values from 0.1 to 1.9
- lift_weight: bfloat16 [2048, 5632], P('sp', 'tp'), may hold values from -0.125 to 0.125
- gate_weight: bfloat16 [2048, 5632], P('sp', 'tp'), may hold values from -0.125 to 0.125
- conv_taps: float32 [3, 5632], P(None, 'tp'), may hold values from -3 to 3
- down_weight: bfloat16 [5632, 2048], P('tp'), may hold values from -0.078125 to 0.078125
Outputs:
- layer_out: bfloat16 [2048, 2048], P(('sp', 'tp'))
The draws below stay inside these ranges and needn't reach their ends.
All inputs are finite; a program needn't handle non-finite values.
Results may differ from the reference program's by a relative error of at most 0.015.
Values may be sent and summed in bfloat16 or wider, within the bound.
A program may use at most 128 MiB of HBM per device.

```python
import math
import jax
import jax.numpy as jnp
from jax import lax

D = 2048
HEADS = 8
HD = 128
VD = 256
FF = 5632
STRETCH = 64
WIDTH = 3
TOKENS = 2048
N_TP = 2


def drawn_pair(key, which):
    base = jax.random.fold_in(key, 71 + which)
    key_draw, query_draw = jax.random.split(base)
    keys = 1.3 * jnp.clip(jax.random.normal(key_draw, (TOKENS, HEADS * HD), jnp.float32), -5.0, 5.0)
    queries = 1.3 * jnp.clip(jax.random.normal(query_draw, (TOKENS, HEADS * HD), jnp.float32), -5.0, 5.0)
    return (queries, keys)


def draw_query_one(key, part):
    return drawn_pair(key, 0)[0].astype(jnp.bfloat16)


def draw_key_one(key, part):
    return drawn_pair(key, 0)[1].astype(jnp.bfloat16)


def draw_query_two(key, part):
    return drawn_pair(key, 1)[0].astype(jnp.bfloat16)


def draw_key_two(key, part):
    return drawn_pair(key, 1)[1].astype(jnp.bfloat16)


def levels(rng, extent, cuts, least, largest):
    def one(axis_at, parts):
        draws = jax.random.uniform(jax.random.fold_in(jax.random.fold_in(rng, 6), axis_at), (parts,), jnp.float32, least / len(cuts), largest / len(cuts))
        return jnp.repeat(jnp.exp(draws), extent[axis_at] // parts).reshape((-1,) + (1,) * (len(extent) - axis_at - 1))

    gain = one(*cuts[0])
    for cut in cuts[1:]:
        gain = gain * one(*cut)
    return gain


def centred(rng, dims, deviation, reach, cuts=(), kind=jnp.bfloat16):
    factor_of = levels(rng, dims, cuts, -0.22, 0.18) if cuts else 1.0
    drawn = jax.random.normal(rng, dims, jnp.float32) * deviation * factor_of
    return jnp.minimum(jnp.maximum(drawn, -reach), reach).astype(kind)


def setup_inputs(seed: int = 0) -> dict:
    key_list = jax.random.split(jax.random.key(seed), 15)
    return {
        "query_one": draw_query_one(jax.random.fold_in(key_list[14], 71), 0),
        "key_one": draw_key_one(jax.random.fold_in(key_list[14], 71), 0),
        "query_two": draw_query_two(jax.random.fold_in(key_list[14], 71), 0),
        "key_two": draw_key_two(jax.random.fold_in(key_list[14], 71), 0),
        "values": centred(key_list[4], (TOKENS, HEADS * VD), 1.0, 6.0, ((0, 16), (1, 2))),
        "mix_weight": jnp.clip(0.3 + 0.5 * jax.random.uniform(key_list[5], (HEADS,), jnp.float32) ** levels(key_list[5], (HEADS,), ((0, 2),), -0.2, 0.2), 0.3, 0.8),
        "head_gain": jnp.clip(1.0 + 0.18 * jax.random.normal(key_list[6], (VD,), jnp.float32), 0.1, 1.9),
        "residual": centred(key_list[7], (TOKENS, D), 1.0, 6.0, ((0, 32),)),
        "out_weight": centred(key_list[8], (HEADS * VD, D), (HEADS * VD) ** -0.5, 0.125, ((0, 2),)),
        "norm_gain": jnp.clip(1.0 + 0.18 * jax.random.normal(key_list[9], (D,), jnp.float32), 0.1, 1.9),
        "lift_weight": centred(key_list[10], (D, FF), D ** -0.5, 0.125, ((0, 16), (1, 2))),
        "gate_weight": centred(key_list[11], (D, FF), D ** -0.5, 0.125, ((0, 16), (1, 2))),
        "conv_taps": centred(key_list[12], (WIDTH, FF), 0.577, 3.0, ((1, 2),), jnp.float32),
        "down_weight": centred(key_list[13], (FF, D), FF ** -0.5, 0.078125, ((0, 2),)),
    }


epsilon = 1e-06
masked_score = -1e+30

def attend_block(first_q, first_k, second_q, second_k, vals, mix_weight, head_gain, start, block_rows):
    scale_factor = HD ** (-0.5)
    q_pos = start + lax.iota(jnp.int32, block_rows)
    k_pos = lax.iota(jnp.int32, TOKENS)
    visible = k_pos[None, :] // STRETCH <= q_pos[:, None] // STRETCH

    def one_map(queries, keys):
        scores = jnp.einsum('thd,shd->hts', queries, keys) * scale_factor
        scores = jnp.where(visible[None], scores, masked_score)
        peak = lax.optimization_barrier(jnp.max(scores, axis=-1, keepdims=True))
        weights = jnp.where(visible[None], jnp.exp(scores - peak), 0.0)
        total = lax.optimization_barrier(jnp.sum(weights, axis=-1))
        rounded = lax.optimization_barrier(weights.astype(jnp.bfloat16))
        acc = jnp.einsum('hts,she->hte', rounded.astype(jnp.float32), vals)
        return acc / total[..., None]
    mixed = one_map(first_q, first_k) - mix_weight[:, None, None] * one_map(second_q, second_k)
    normed = mixed * lax.rsqrt(lax.optimization_barrier(jnp.mean(mixed * mixed, axis=-1, keepdims=True)) + epsilon) * head_gain
    return jnp.transpose(normed.astype(jnp.bfloat16), (1, 0, 2))

def reference(query_one, key_one, query_two, key_two, values, mix_weight, head_gain, residual, out_weight, norm_gain, lift_weight, gate_weight, conv_taps, down_weight):
    val_width = 2 * HD
    block_rows = math.gcd(TOKENS, 512)
    blocks = TOKENS // block_rows
    q_one = query_one.astype(jnp.float32).reshape(TOKENS, HEADS, HD)
    q_two = query_two.astype(jnp.float32).reshape(TOKENS, HEADS, HD)
    k_one = key_one.astype(jnp.float32).reshape(TOKENS, HEADS, HD)
    k_two = key_two.astype(jnp.float32).reshape(TOKENS, HEADS, HD)
    vals = values.astype(jnp.float32).reshape(TOKENS, HEADS, val_width)

    def per_block(index):
        start = (index * block_rows).astype(jnp.int32)
        first_q = lax.dynamic_slice_in_dim(q_one, start, block_rows, 0)
        second_q = lax.dynamic_slice_in_dim(q_two, start, block_rows, 0)
        return attend_block(first_q, k_one, second_q, k_two, vals, mix_weight, head_gain, start, block_rows)
    head_out = lax.map(per_block, jnp.arange(blocks, dtype=jnp.int32))
    head_out = head_out.reshape(TOKENS, HEADS * val_width)
    group = HEADS * val_width // N_TP
    attended = jnp.zeros((TOKENS, D), jnp.float32)
    for index in range(N_TP):
        partial_sum = jnp.dot(head_out[:, index * group:(index + 1) * group], out_weight[index * group:(index + 1) * group], preferred_element_type=jnp.float32)
        attended = attended + partial_sum.astype(jnp.bfloat16).astype(jnp.float32)
    stream = residual.astype(jnp.float32) + attended
    normed = (stream * lax.rsqrt(lax.optimization_barrier(jnp.mean(stream * stream, axis=-1, keepdims=True)) + epsilon) * norm_gain).astype(jnp.bfloat16)
    lifted = jnp.dot(normed, lift_weight, preferred_element_type=jnp.float32).astype(jnp.bfloat16)
    gated = jnp.dot(normed, gate_weight, preferred_element_type=jnp.float32).astype(jnp.bfloat16)
    padded = jnp.concatenate([jnp.zeros((WIDTH - 1, FF), jnp.float32), gated.astype(jnp.float32)], axis=0)
    conv = jnp.zeros((TOKENS, FF), jnp.float32)
    for index in range(WIDTH):
        conv = conv + conv_taps[index] * padded[index:index + TOKENS]
    hidden = (jax.nn.silu(conv) * lifted.astype(jnp.float32)).astype(jnp.bfloat16)
    units = FF // N_TP
    mixer = jnp.zeros((TOKENS, D), jnp.float32)
    for index in range(N_TP):
        partial_sum = jnp.dot(hidden[:, index * units:(index + 1) * units], down_weight[index * units:(index + 1) * units], preferred_element_type=jnp.float32)
        mixer = mixer + partial_sum.astype(jnp.bfloat16).astype(jnp.float32)
    return (stream + mixer).astype(jnp.bfloat16)
```

```python
import functools

import jax
import jax.numpy as jnp
from jax import lax
from jax.experimental import pallas as pl
from jax.experimental.pallas import tpu as pltpu
from jax.sharding import PartitionSpec as P

HD = 128
STRETCH = 64
WIDTH = 3


epsilon = 1e-06
masked_score = -1e30


def passed_along(block, axis, distance):
    devices = range(lax.axis_size(axis))
    route = [(i - distance, i) for i in devices if i - distance in devices]
    return lax.ppermute(block, axis, route)


def update_map(peak, total, acc, queries, keys, vals, visible):
    scores = jnp.einsum("thd,shd->hts", queries, keys, preferred_element_type=jnp.float32) * HD ** (
        -0.5
    )
    scores = jnp.where(visible[None], scores, masked_score)
    new_peak = jnp.maximum(peak, jnp.max(scores, axis=-1))
    weights = jnp.where(visible[None], jnp.exp(scores - new_peak[..., None]), 0.0)
    total = jnp.sum(weights, axis=-1)
    acc = jnp.einsum(
        "hts,she->hte", weights.astype(jnp.bfloat16), vals, preferred_element_type=jnp.float32
    )
    return (new_peak, total, acc)


def on_device(
    query_one,
    key_one,
    query_two,
    key_two,
    values,
    mix_weight,
    head_gain,
    residual,
    out_weight,
    norm_gain,
    lift_weight,
    gate_weight,
    conv_taps,
    down_weight,
):
    tok_local = query_one.shape[0]
    heads_local = mix_weight.shape[0]
    val_width = values.shape[1] // heads_local
    model_width = residual.shape[1]
    offset = lax.axis_index("sp") * tok_local
    q_pos = offset + lax.iota(jnp.int32, tok_local)
    q_one = query_one.reshape(tok_local, heads_local, HD)
    q_two = query_two.reshape(tok_local, heads_local, HD)
    start_peak = jnp.full((heads_local, tok_local), masked_score, jnp.float32)
    start_total = jnp.zeros((heads_local, tok_local), jnp.float32)
    start_acc = jnp.zeros((heads_local, tok_local, val_width), jnp.float32)
    initial = (start_peak, start_total, start_acc, start_peak, start_total, start_acc)
    first_keys = lax.all_gather(key_one, "sp", axis=0, tiled=True)
    second_keys = lax.all_gather(key_two, "sp", axis=0, tiled=True)
    piece_vals = lax.all_gather(values, "sp", axis=0, tiled=True)
    count = first_keys.shape[0]
    k_pos = lax.iota(jnp.int32, count)
    visible = k_pos[None, :] // STRETCH <= q_pos[:, None] // STRETCH
    first_keys = first_keys.reshape(count, heads_local, HD)
    second_keys = second_keys.reshape(count, heads_local, HD)
    piece_vals = piece_vals.reshape(count, heads_local, val_width)
    first = update_map(initial[0], initial[1], initial[2], q_one, first_keys, piece_vals, visible)
    second = update_map(initial[3], initial[4], initial[5], q_two, second_keys, piece_vals, visible)
    state = first + second
    mixed = (
        state[2] / state[1][..., None] - mix_weight[:, None, None] * state[5] / state[4][..., None]
    )
    head_out = (
        mixed * lax.rsqrt(jnp.mean(mixed * mixed, axis=-1, keepdims=True) + epsilon) * head_gain
    ).astype(jnp.bfloat16)
    out_heads = out_weight.reshape(heads_local, val_width, model_width)
    piece = head_out
    attended = lax.psum_scatter(
        jnp.einsum("hte,hed->td", piece, out_heads, preferred_element_type=jnp.float32).astype(
            jnp.bfloat16
        ),
        "tp",
        scatter_dimension=0,
        tiled=True,
    ).astype(jnp.float32)
    stream = residual.astype(jnp.float32) + attended
    normed = (
        stream * lax.rsqrt(jnp.mean(stream * stream, axis=-1, keepdims=True) + epsilon) * norm_gain
    ).astype(jnp.bfloat16)
    whole_rows = lax.all_gather(normed, "tp", axis=0, tiled=True)
    lift_pre = jnp.dot(
        whole_rows,
        lax.all_gather(lift_weight, "sp", axis=0, tiled=True),
        preferred_element_type=jnp.float32,
    )
    gate_pre = jnp.dot(
        whole_rows,
        lax.all_gather(gate_weight, "sp", axis=0, tiled=True),
        preferred_element_type=jnp.float32,
    )
    lifted = lift_pre.astype(jnp.bfloat16)
    gated = gate_pre.astype(jnp.bfloat16)
    prior = passed_along(gated[tok_local - (WIDTH - 1) :], "sp", 1)
    extended = jnp.concatenate([prior, gated], axis=0).astype(jnp.float32)
    conv = conv_taps[0] * extended[0:tok_local]
    for index in range(1, WIDTH):
        conv = conv + conv_taps[index] * extended[index : index + tok_local]
    hidden = (jax.nn.silu(conv) * lifted.astype(jnp.float32)).astype(jnp.bfloat16)
    piece = hidden
    mixer = lax.psum_scatter(
        jnp.dot(piece, down_weight, preferred_element_type=jnp.float32).astype(jnp.bfloat16),
        "tp",
        scatter_dimension=0,
        tiled=True,
    ).astype(jnp.float32)
    return (stream + mixer).astype(jnp.bfloat16)

MESH = pl.DeviceIdType.MESH


def remote(src, dst, send_sem, recv_sem, sp, tp):
    return pltpu.make_async_remote_copy(
        src_ref=src,
        dst_ref=dst,
        send_sem=send_sem,
        recv_sem=recv_sem,
        device_id=(sp, tp),
        device_id_type=MESH,
    )


def greet(peers, count=None):
    barrier = pltpu.get_barrier_semaphore()
    for peer in peers:
        pl.semaphore_signal(barrier, inc=1, device_id=peer, device_id_type=MESH)
    pl.semaphore_wait(barrier, len(peers) if count is None else count)


def block_of(index, size):
    return pl.ds(pl.multiple_of(index * size, size), size)


def spread_kernel(
    plane, planes, width, q1, k1, q2, k2, v, lift, gate,
    q_all, kv_all, lift_all, gate_all,
    own_sem, a_send, a_recv, w_send, w_recv, kv_send, kv_recv, g_send, g_recv,
):
    sp, tp = lax.axis_index("sp"), lax.axis_index("tp")
    z, p = sp // plane, sp % plane
    tok = q1.shape[0]
    tiles = lift.shape[1] // 128
    greet(
        [(z * plane + (p + d) % plane, tp) for d in range(1, plane)]
        + [((z + d) % planes * plane + p, tp) for d in range(1, planes)]
    )

    def piece(head, row):
        h1, h2 = block_of(head, HD), block_of(head, 2 * HD)
        rows, all_rows = block_of(row % plane, tok), block_of(row, tok)
        return [
            (q1.at[:, h1], q_all.at[rows, 0:HD]),
            (q2.at[:, h1], q_all.at[rows, HD : 2 * HD]),
            (k1.at[:, h1], kv_all.at[all_rows, 0:HD]),
            (k2.at[:, h1], kv_all.at[all_rows, HD : 2 * HD]),
            (v.at[:, h2], kv_all.at[all_rows, 2 * HD : 4 * HD]),
        ]

    def units(index):
        return pl.ds(pl.multiple_of(index * tiles // planes * 128, 128), width)

    started = []
    own = []
    for n, (src, dst) in enumerate(piece(p, sp)):
        own.append(pltpu.make_async_copy(src, dst, own_sem.at[n]))
    for m, (src, dst) in enumerate(((lift, lift_all), (gate, gate_all))):
        own.append(
            pltpu.make_async_copy(src.at[:, units(z)], dst.at[block_of(sp, tok), :], own_sem.at[5 + m])
        )
    for copy in own:
        copy.start()
    for d in range(1, plane):
        there = (p + d) % plane
        for n, (src, dst) in enumerate(piece(there, sp)):
            copy = remote(src, dst, a_send.at[d, n], a_recv.at[d, n], z * plane + there, tp)
            copy.start()
            started.append(copy)
    for d in range(1, planes):
        there = (z + d) % planes
        for m, (src, dst) in enumerate(((lift, lift_all), (gate, gate_all))):
            copy = remote(
                src.at[:, units(there)], dst.at[block_of(sp, tok), :],
                w_send.at[d, m], w_recv.at[d, m], there * plane + p, tp,
            )
            copy.start()
            started.append(copy)
    for m, (src, dst) in enumerate(((lift, lift_all), (gate, gate_all))):
        for e in range(1, plane):
            copy = remote(
                src.at[:, units(z)], dst.at[block_of(sp, tok), :],
                g_send.at[0, e, m], g_recv.at[0, e, m], z * plane + (p + e) % plane, tp,
            )
            copy.start()
            started.append(copy)
    for copy in own:
        copy.wait()
    for d in range(1, plane):
        source = z * plane + (p + plane - d) % plane
        for n, (src, dst) in enumerate(piece(p, source)):
            remote(src, dst, a_send.at[d, n], a_recv.at[d, n], source, tp).wait_recv()
    mine = kv_all.at[block_of(z, plane * tok), :]
    for d in range(1, planes):

        @pl.when(z + d < planes)
        def _():
            remote(mine, mine, kv_send.at[d], kv_recv.at[d], (z + d) % planes * plane + p, tp).start()

    for d in range(1, planes):
        source = (z + planes - d) % planes * plane + p
        rows = block_of(source, tok)
        for m, dst in enumerate((lift_all, gate_all)):
            remote(dst.at[rows, :], dst.at[rows, :], w_send.at[d, m], w_recv.at[d, m], source, tp).wait_recv()
            for e in range(1, plane):
                copy = remote(
                    dst.at[rows, :], dst.at[rows, :],
                    g_send.at[d, e, m], g_recv.at[d, e, m], z * plane + (p + e) % plane, tp,
                )
                copy.start()
                started.append(copy)
    for d in range(planes):
        for e in range(1, plane):
            there = (p + plane - e) % plane
            rows = block_of((z + planes - d) % planes * plane + there, tok)
            for m, dst in enumerate((lift_all, gate_all)):
                remote(
                    dst.at[rows, :], dst.at[rows, :], g_send.at[d, e, m], g_recv.at[d, e, m],
                    z * plane + there, tp,
                ).wait_recv()
    for d in range(1, planes):
        below = kv_all.at[block_of((z + planes - d) % planes, plane * tok), :]

        @pl.when(z - d >= 0)
        def _():
            remote(below, below, kv_send.at[d], kv_recv.at[d], sp, tp).wait_recv()

        @pl.when(z + d < planes)
        def _():
            remote(mine, mine, kv_send.at[d], kv_recv.at[d], sp, tp).wait_send()

    for copy in started:
        copy.wait_send()


def out_kernel(
    plane, planes, head_out, out_weight, residual, gain,
    normed, halo, stream,
    heads, part, part_in, tail, own_sem, a_send, a_recv, t_send, t_recv,
    z_send, z_recv, f_send, f_recv, h_send, h_recv,
):
    sp, tp = lax.axis_index("sp"), lax.axis_index("tp")
    z, p = sp // plane, sp % plane
    other = 1 - tp
    tok = heads.shape[1]
    half = tok // 2
    val = heads.shape[2]
    before = (p + plane - 1) % plane
    peers = (
        [(z * plane + (p + d) % plane, tp) for d in range(1, plane)]
        + [((z + d) % planes * plane + p, tp) for d in range(1, planes)]
        + [(sp, other)]
    )
    barrier = pltpu.get_barrier_semaphore()
    for peer in peers + [(s * plane + before, 1) for s in range(planes)]:
        pl.semaphore_signal(barrier, inc=1, device_id=peer, device_id_type=MESH)
    pl.semaphore_wait(barrier, len(peers) + 2 * planes * tp)

    started = []
    own = pltpu.make_async_copy(head_out.at[block_of(p, tok), :], heads.at[p], own_sem)
    own.start()
    for d in range(1, plane):
        there = (p + d) % plane
        copy = remote(
            head_out.at[block_of(there, tok), :], heads.at[p],
            a_send.at[d], a_recv.at[d], z * plane + there, tp,
        )
        copy.start()
        started.append(copy)
    own.wait()
    for d in range(1, plane):
        there = (p + plane - d) % plane
        remote(
            heads.at[there], heads.at[there], a_send.at[d], a_recv.at[d], z * plane + there, tp
        ).wait_recv()

    columns = 512

    def product(which, at):
        total = None
        for h in range(plane):
            term = jnp.dot(
                heads[h, block_of(which, half), :],
                out_weight[h * val : (h + 1) * val, at : at + columns],
                preferred_element_type=jnp.float32,
            )
            total = term if total is None else total + term
        return total.astype(jnp.bfloat16)

    model = out_weight.shape[1]
    for at in range(0, model, columns):
        part[:, at : at + columns] = product(other, at)
    swap = remote(part, part_in, t_send, t_recv, sp, other)
    swap.start()
    started.append(swap)
    for at in range(0, model, columns):
        stream[:, at : at + columns] = product(tp, at).astype(jnp.float32)
    swap.wait_recv()
    whole = residual[...].astype(jnp.float32) + (stream[...] + part_in[...].astype(jnp.float32))
    stream[...] = whole
    scaled = whole * lax.rsqrt(jnp.mean(whole * whole, axis=-1, keepdims=True) + epsilon) * gain[...]
    rounded = scaled.astype(jnp.bfloat16)
    normed[z, block_of(tp, half), :] = rounded
    tail[...] = scaled[half - 8 :, :].astype(jnp.bfloat16)

    mine = normed.at[z, block_of(tp, half), :]
    for d in range(1, planes):
        copy = remote(mine, mine, z_send.at[d], z_recv.at[d], (z + d) % planes * plane + p, tp)
        copy.start()
        started.append(copy)
    copy = remote(mine, mine, f_send.at[0], f_recv.at[0], sp, other)
    copy.start()
    started.append(copy)
    after = (p + 1) % plane
    zone = z + (p + 1) // plane

    @pl.when(jnp.logical_and(tp == 1, zone < planes))
    def _():
        for s in range(planes):
            for t in range(2):
                remote(
                    tail, halo.at[zone], h_send.at[s, t], h_recv.at[zone], s * plane + after, t
                ).start()

    for d in range(1, planes):
        there = (z + planes - d) % planes
        theirs = normed.at[there, block_of(tp, half), :]
        remote(theirs, theirs, z_send.at[d], z_recv.at[d], sp, other).wait_recv()
        copy = remote(theirs, theirs, f_send.at[d], f_recv.at[d], sp, other)
        copy.start()
        started.append(copy)
    for d in range(planes):
        theirs = normed.at[(z + planes - d) % planes, block_of(other, half), :]
        remote(theirs, theirs, f_send.at[d], f_recv.at[d], sp, other).wait_recv()
    for s in range(planes):

        @pl.when(s * plane + p > 0)
        def _():
            remote(tail, halo.at[s], h_send.at[s, 0], h_recv.at[s], sp, other).wait_recv()

        @pl.when(s * plane + p == 0)
        def _():
            halo[s] = jnp.zeros(halo.shape[1:], halo.dtype)

    @pl.when(jnp.logical_and(tp == 1, zone < planes))
    def _():
        for s in range(planes):
            for t in range(2):
                remote(tail, halo.at[0], h_send.at[s, t], h_recv.at[0], sp, other).wait_send()

    for copy in started:
        copy.wait_send()


def down_kernel(
    plane, planes, starts, hidden, weight, stream, out,
    units, total_buf, part, part_in, own_sem, a_send, a_recv, t_send, t_recv,
):
    sp, tp = lax.axis_index("sp"), lax.axis_index("tp")
    z, p = sp // plane, sp % plane
    other = 1 - tp
    tok = units.shape[1]
    half = tok // 2
    greet([((z + d) % planes * plane + p, tp) for d in range(1, planes)] + [(sp, other)])
    started = []
    own = pltpu.make_async_copy(hidden.at[z], units.at[z], own_sem)
    own.start()
    for d in range(1, planes):
        there = (z + d) % planes
        copy = remote(
            hidden.at[there], units.at[z], a_send.at[d], a_recv.at[d], there * plane + p, tp
        )
        copy.start()
        started.append(copy)
    own.wait()
    for d in range(1, planes):
        there = (z + planes - d) % planes
        remote(
            units.at[there], units.at[there], a_send.at[d], a_recv.at[d], sp, other
        ).wait_recv()
    model = weight.shape[1]
    columns = 256

    def product(which, at):
        total = None
        for s in range(planes):
            term = jnp.dot(
                units[s, block_of(which, half), 0 : starts[s + 1] - starts[s]],
                weight[starts[s] : starts[s + 1], block_of(at, columns)],
                preferred_element_type=jnp.float32,
            )
            total = term if total is None else total + term
        return total.astype(jnp.bfloat16)

    @pl.loop(0, model // columns)
    def _(at):
        part[:, block_of(at, columns)] = product(other, at)

    swap = remote(part, part_in, t_send, t_recv, sp, other)
    swap.start()
    started.append(swap)

    @pl.loop(0, model // columns)
    def _(at):
        here = block_of(at, columns)
        total_buf[:, here] = stream[:, here] + product(tp, at).astype(jnp.float32)

    swap.wait_recv()
    out[...] = (total_buf[...] + part_in[...].astype(jnp.float32)).astype(out.dtype)
    for copy in started:
        copy.wait_send()


def shorter_routes(
    plane, planes,
    query_one, key_one, query_two, key_two, values, mix_weight, head_gain, residual, out_weight,
    norm_gain, lift_weight, gate_weight, conv_taps, down_weight,
):
    bf16, f32 = jnp.bfloat16, jnp.float32
    tok = query_one.shape[0]
    model = residual.shape[1]
    val = 2 * HD
    ff = lift_weight.shape[1]
    tiles = ff // 128
    starts = [s * tiles // planes * 128 for s in range(planes + 1)]
    width = -(-tiles // planes) * 128
    count = planes * plane * tok
    sp = lax.axis_index("sp")
    z, p = sp // plane, sp % plane
    dma = pltpu.SemaphoreType.DMA
    anywhere = pl.BlockSpec(memory_space=pl.ANY)
    local = pl.BlockSpec(memory_space=pltpu.VMEM)
    shape = jax.ShapeDtypeStruct

    q_all, kv_all, lift_all, gate_all = pl.pallas_call(
        functools.partial(spread_kernel, plane, planes, width),
        out_shape=(
            shape((plane * tok, 2 * HD), bf16),
            shape((count, 4 * HD), bf16),
            shape((count, width), bf16),
            shape((count, width), bf16),
        ),
        in_specs=[anywhere] * 7,
        out_specs=(anywhere,) * 4,
        scratch_shapes=[
            dma((7,)), dma((plane, 5)), dma((plane, 5)), dma((planes, 2)), dma((planes, 2)),
            dma((planes,)), dma((planes,)), dma((planes, plane, 2)), dma((planes, plane, 2)),
        ],
        compiler_params=pltpu.CompilerParams(collective_id=0, has_side_effects=True),
        name="spread",
    )(query_one, key_one, query_two, key_two, values, lift_weight, gate_weight)

    k_pos = lax.iota(jnp.int32, count)
    q_pos = z * plane * tok + lax.iota(jnp.int32, plane * tok)
    visible = k_pos[None, :] // STRETCH <= q_pos[:, None] // STRETCH
    arrived = k_pos[:, None] < (z + 1) * plane * tok
    vals = jnp.where(arrived, kv_all[:, 2 * HD :], 0)

    def one_map(index):
        queries = q_all[:, index * HD : (index + 1) * HD]
        keys = kv_all[:, index * HD : (index + 1) * HD]
        scores = jnp.einsum("td,sd->ts", queries, keys, preferred_element_type=f32) * HD**-0.5
        scores = jnp.where(visible, scores, masked_score)
        weights = jnp.where(visible, jnp.exp(scores - jnp.max(scores, axis=-1, keepdims=True)), 0.0)
        total = jnp.sum(weights, axis=-1, keepdims=True)
        return jnp.dot(weights.astype(bf16), vals, preferred_element_type=f32) / total

    mixed = one_map(0) - mix_weight[p] * one_map(1)
    head_out = (
        mixed * lax.rsqrt(jnp.mean(mixed * mixed, axis=-1, keepdims=True) + epsilon) * head_gain
    ).astype(bf16)

    normed, halo, stream = pl.pallas_call(
        functools.partial(out_kernel, plane, planes),
        out_shape=(
            shape((planes, tok, model), bf16),
            shape((planes, 8, model), bf16),
            shape((tok // 2, model), f32),
        ),
        in_specs=[local] * 4,
        out_specs=(local,) * 3,
        scratch_shapes=[
            pltpu.VMEM((plane, tok, val), bf16),
            pltpu.VMEM((tok // 2, model), bf16),
            pltpu.VMEM((tok // 2, model), bf16),
            pltpu.VMEM((8, model), bf16),
            dma, dma((plane,)), dma((plane,)), dma, dma,
            dma((planes,)), dma((planes,)), dma((planes,)), dma((planes,)),
            dma((planes, 2)), dma((planes,)),
        ],
        compiler_params=pltpu.CompilerParams(
            collective_id=1, has_side_effects=True, vmem_limit_bytes=32 << 20
        ),
        name="project",
    )(head_out, out_weight, residual, norm_gain.reshape(1, model))

    rows = jnp.concatenate([halo, normed], axis=1).reshape(planes * (tok + 8), model)
    lifted = jnp.dot(rows, lift_all, preferred_element_type=f32).astype(bf16)
    gated = jnp.dot(rows, gate_all, preferred_element_type=f32).astype(bf16)
    lifted = lifted.reshape(planes, tok + 8, width)[:, 8:].astype(f32)
    gated = gated.reshape(planes, tok + 8, width).astype(f32)
    taps = lax.dynamic_slice_in_dim(conv_taps, z * tiles // planes * 128, width, 1)
    conv = 0.0
    for index in range(WIDTH):
        at = 8 - (WIDTH - 1) + index
        conv = conv + taps[index] * gated[:, at : at + tok]
    hidden = (jax.nn.silu(conv) * lifted).astype(bf16)

    return pl.pallas_call(
        functools.partial(down_kernel, plane, planes, starts),
        out_shape=shape((tok // 2, model), bf16),
        in_specs=[local] * 3,
        out_specs=local,
        scratch_shapes=[
            pltpu.VMEM((planes, tok, width), bf16),
            pltpu.VMEM((tok // 2, model), f32),
            pltpu.VMEM((tok // 2, model), bf16),
            pltpu.VMEM((tok // 2, model), bf16),
            dma, dma((planes,)), dma((planes,)), dma, dma,
        ],
        compiler_params=pltpu.CompilerParams(
            collective_id=2, has_side_effects=True, vmem_limit_bytes=40 << 20
        ),
        name="down",
    )(hidden, down_weight, stream)


def any_route(*arrays):
    tok, heads, ff = arrays[0].shape[0], arrays[5].shape[0], arrays[10].shape[1]
    devices, groups = lax.axis_size("sp"), lax.axis_size("tp")
    planes = devices // heads
    fits = (
        groups == 2 and heads > 1 and planes > 1 and devices % heads == 0
        and ff % 128 == 0 and tok % 128 == 0 and WIDTH <= 9
        and arrays[10].shape[0] == tok
    )
    if fits:
        return shorter_routes(heads, planes, *arrays)
    return on_device(*arrays)


def solution(mesh):
    return jax.shard_map(
        any_route,
        mesh=mesh,
        in_specs=(
            P("sp", "tp"),
            P("sp", "tp"),
            P("sp", "tp"),
            P("sp", "tp"),
            P("sp", "tp"),
            P("tp"),
            P(),
            P(("sp", "tp"), None),
            P("tp", None),
            P(),
            P("sp", "tp"),
            P("sp", "tp"),
            P(None, "tp"),
            P("tp", None),
        ),
        out_specs=P(("sp", "tp"), None),
        check_vma=False,
    )
```

```python
import functools

import jax
import jax.numpy as jnp
from jax import lax
from jax.experimental import pallas as pl
from jax.experimental.pallas import tpu as pltpu
from jax.sharding import PartitionSpec as P

HD = 128
STRETCH = 64
WIDTH = 3


epsilon = 1e-06
masked_score = -1e30


def passed_along(block, axis, distance):
    devices = range(lax.axis_size(axis))
    route = [(i - distance, i) for i in devices if i - distance in devices]
    return lax.ppermute(block, axis, route)


def update_map(peak, total, acc, queries, keys, vals, visible):
    scores = jnp.einsum("thd,shd->hts", queries, keys, preferred_element_type=jnp.float32) * HD ** (
        -0.5
    )
    scores = jnp.where(visible[None], scores, masked_score)
    new_peak = jnp.maximum(peak, jnp.max(scores, axis=-1))
    weights = jnp.where(visible[None], jnp.exp(scores - new_peak[..., None]), 0.0)
    total = jnp.sum(weights, axis=-1)
    acc = jnp.einsum(
        "hts,she->hte", weights.astype(jnp.bfloat16), vals, preferred_element_type=jnp.float32
    )
    return (new_peak, total, acc)


def on_device(
    query_one,
    key_one,
    query_two,
    key_two,
    values,
    mix_weight,
    head_gain,
    residual,
    out_weight,
    norm_gain,
    lift_weight,
    gate_weight,
    conv_taps,
    down_weight,
):
    tok_local = query_one.shape[0]
    heads_local = mix_weight.shape[0]
    val_width = values.shape[1] // heads_local
    model_width = residual.shape[1]
    offset = lax.axis_index("sp") * tok_local
    q_pos = offset + lax.iota(jnp.int32, tok_local)
    q_one = query_one.reshape(tok_local, heads_local, HD)
    q_two = query_two.reshape(tok_local, heads_local, HD)
    start_peak = jnp.full((heads_local, tok_local), masked_score, jnp.float32)
    start_total = jnp.zeros((heads_local, tok_local), jnp.float32)
    start_acc = jnp.zeros((heads_local, tok_local, val_width), jnp.float32)
    initial = (start_peak, start_total, start_acc, start_peak, start_total, start_acc)
    first_keys = lax.all_gather(key_one, "sp", axis=0, tiled=True)
    second_keys = lax.all_gather(key_two, "sp", axis=0, tiled=True)
    piece_vals = lax.all_gather(values, "sp", axis=0, tiled=True)
    count = first_keys.shape[0]
    k_pos = lax.iota(jnp.int32, count)
    visible = k_pos[None, :] // STRETCH <= q_pos[:, None] // STRETCH
    first_keys = first_keys.reshape(count, heads_local, HD)
    second_keys = second_keys.reshape(count, heads_local, HD)
    piece_vals = piece_vals.reshape(count, heads_local, val_width)
    first = update_map(initial[0], initial[1], initial[2], q_one, first_keys, piece_vals, visible)
    second = update_map(initial[3], initial[4], initial[5], q_two, second_keys, piece_vals, visible)
    state = first + second
    mixed = (
        state[2] / state[1][..., None] - mix_weight[:, None, None] * state[5] / state[4][..., None]
    )
    head_out = (
        mixed * lax.rsqrt(jnp.mean(mixed * mixed, axis=-1, keepdims=True) + epsilon) * head_gain
    ).astype(jnp.bfloat16)
    out_heads = out_weight.reshape(heads_local, val_width, model_width)
    piece = head_out
    attended = lax.psum_scatter(
        jnp.einsum("hte,hed->td", piece, out_heads, preferred_element_type=jnp.float32).astype(
            jnp.bfloat16
        ),
        "tp",
        scatter_dimension=0,
        tiled=True,
    ).astype(jnp.float32)
    stream = residual.astype(jnp.float32) + attended
    normed = (
        stream * lax.rsqrt(jnp.mean(stream * stream, axis=-1, keepdims=True) + epsilon) * norm_gain
    ).astype(jnp.bfloat16)
    whole_rows = lax.all_gather(normed, "tp", axis=0, tiled=True)
    lift_pre = jnp.dot(
        whole_rows,
        lax.all_gather(lift_weight, "sp", axis=0, tiled=True),
        preferred_element_type=jnp.float32,
    )
    gate_pre = jnp.dot(
        whole_rows,
        lax.all_gather(gate_weight, "sp", axis=0, tiled=True),
        preferred_element_type=jnp.float32,
    )
    lifted = lift_pre.astype(jnp.bfloat16)
    gated = gate_pre.astype(jnp.bfloat16)
    prior = passed_along(gated[tok_local - (WIDTH - 1) :], "sp", 1)
    extended = jnp.concatenate([prior, gated], axis=0).astype(jnp.float32)
    conv = conv_taps[0] * extended[0:tok_local]
    for index in range(1, WIDTH):
        conv = conv + conv_taps[index] * extended[index : index + tok_local]
    hidden = (jax.nn.silu(conv) * lifted.astype(jnp.float32)).astype(jnp.bfloat16)
    piece = hidden
    mixer = lax.psum_scatter(
        jnp.dot(piece, down_weight, preferred_element_type=jnp.float32).astype(jnp.bfloat16),
        "tp",
        scatter_dimension=0,
        tiled=True,
    ).astype(jnp.float32)
    return (stream + mixer).astype(jnp.bfloat16)

MESH = pl.DeviceIdType.MESH


def remote(src, dst, send_sem, recv_sem, sp, tp):
    return pltpu.make_async_remote_copy(
        src_ref=src,
        dst_ref=dst,
        send_sem=send_sem,
        recv_sem=recv_sem,
        device_id=(sp, tp),
        device_id_type=MESH,
    )


def greet(peers, count=None):
    barrier = pltpu.get_barrier_semaphore()
    for peer in peers:
        pl.semaphore_signal(barrier, inc=1, device_id=peer, device_id_type=MESH)
    pl.semaphore_wait(barrier, len(peers) if count is None else count)


def block_of(index, size):
    return pl.ds(pl.multiple_of(index * size, size), size)


def front_kernel(
    plane, planes, width, q1, k1, q2, k2, v, lift, gate, mix_weight, head_gain, out_weight, residual,
    gain,
    lift_all, gate_all, normed, halo, stream,
    q_all, kv_all, peaks, totals, sums, head_out, heads, part, part_in, tail,
    own_sem, a_send, a_recv, w_send, w_recv, kv_send, kv_recv, g_send, g_recv,
    b_own, b_send, b_recv, t_send, t_recv, up_send, up_recv, down_send, down_recv,
    f_send, f_recv, h_send, h_recv,
):
    sp, tp = lax.axis_index("sp"), lax.axis_index("tp")
    z, p = sp // plane, sp % plane
    other = 1 - tp
    tok = q1.shape[0]
    half = tok // 2
    val = 2 * HD
    tiles = lift.shape[1] // 128
    before = (p + plane - 1) % plane
    above, below = (z + 1) % planes * plane + p, (z + planes - 1) % planes * plane + p
    weights = ((lift, lift_all), (gate, gate_all))
    peers = (
        [(z * plane + (p + d) % plane, tp) for d in range(1, plane)]
        + [((z + d) % planes * plane + p, tp) for d in range(1, planes)]
        + [(sp, other)]
    )
    barrier = pltpu.get_barrier_semaphore()
    for peer in peers + [(s * plane + before, 1) for s in range(planes)]:
        pl.semaphore_signal(barrier, inc=1, device_id=peer, device_id_type=MESH)

    def piece(head, row):
        h1, h2 = block_of(head, HD), block_of(head, 2 * HD)
        rows, all_rows = block_of(row % plane, tok), block_of(row, tok)
        return [
            (k1.at[:, h1], kv_all.at[all_rows, 0:HD]),
            (k2.at[:, h1], kv_all.at[all_rows, HD : 2 * HD]),
            (v.at[:, h2], kv_all.at[all_rows, 2 * HD : 4 * HD]),
            (q1.at[:, h1], q_all.at[rows, 0:HD]),
            (q2.at[:, h1], q_all.at[rows, HD : 2 * HD]),
        ]

    def units(index):
        return pl.ds(pl.multiple_of(index * tiles // planes * 128, 128), width)

    started = []
    own = [
        pltpu.make_async_copy(src, dst, own_sem.at[n]) for n, (src, dst) in enumerate(piece(p, sp))
    ]
    own_weights = [
        pltpu.make_async_copy(src.at[:, units(z)], dst.at[block_of(sp, tok), :], own_sem.at[5 + m])
        for m, (src, dst) in enumerate(weights)
    ]
    for copy in own:
        copy.start()
    pl.semaphore_wait(barrier, len(peers) + 2 * planes * tp)
    for d in range(1, plane):
        there = (p + d) % plane
        for n, (src, dst) in enumerate(piece(there, sp)):
            copy = remote(src, dst, a_send.at[d, n], a_recv.at[d, n], z * plane + there, tp)
            copy.start()
            started.append(copy)

    def send_weights(d):
        there = (z + d) % planes
        for m, (src, dst) in enumerate(weights):
            copy = remote(
                src.at[:, units(there)], dst.at[block_of(sp, tok), :],
                w_send.at[d, m], w_recv.at[d, m], there * plane + p, tp,
            )
            copy.start()
            started.append(copy)

    def share_weights(d):
        source = (z + planes - d) % planes * plane + p
        rows = block_of(source, tok)
        for m, dst in enumerate((lift_all, gate_all)):
            if d:
                remote(
                    dst.at[rows, :], dst.at[rows, :], w_send.at[d, m], w_recv.at[d, m], source, tp
                ).wait_recv()
            src = dst.at[rows, :] if d else weights[m][0].at[:, units(z)]
            for e in range(1, plane):
                copy = remote(
                    src, dst.at[rows, :], g_send.at[d, e, m], g_recv.at[d, e, m],
                    z * plane + (p + e) % plane, tp,
                )
                copy.start()
                started.append(copy)

    if planes > 2:
        send_weights(planes - 1)
    share_weights(0)
    for copy in own_weights:
        copy.start()
    for copy in own:
        copy.wait()
    for d in range(1, plane):
        source = z * plane + (p + plane - d) % plane
        for n, (src, dst) in enumerate(piece(p, source)):
            remote(src, dst, a_send.at[d, n], a_recv.at[d, n], source, tp).wait_recv()

    span = plane * tok

    def keys_of(index):
        return kv_all.at[block_of(index, span), :]

    @pl.when(z + 1 < planes)
    def _():
        remote(keys_of(z), keys_of(z), kv_send.at[1], kv_recv.at[1], above, tp).start()

    def attend(source, first):
        @pl.loop(0, plane)
        def _(chunk):
            rows, keys = block_of(chunk, tok), block_of(source, span)
            for m in range(2):
                scores = lax.dot_general(
                    q_all[rows, m * HD : (m + 1) * HD],
                    kv_all[keys, m * HD : (m + 1) * HD],
                    (((1,), (1,)), ((), ())),
                    preferred_element_type=jnp.float32,
                ) * HD ** (-0.5)
                if first:
                    k_pos = lax.broadcasted_iota(jnp.int32, (tok, span), 1)
                    q_pos = chunk * tok + lax.broadcasted_iota(jnp.int32, (tok, span), 0)
                    visible = lax.div(k_pos, STRETCH) <= lax.div(q_pos, STRETCH)
                    scores = jnp.where(visible, scores, masked_score)
                    peak = jnp.max(scores, axis=-1, keepdims=True)
                    terms = jnp.where(visible, jnp.exp(scores - peak), 0.0)
                else:
                    last = peaks[m, rows, 0:1]
                    peak = jnp.maximum(last, jnp.max(scores, axis=-1, keepdims=True))
                    terms = jnp.exp(scores - peak)
                total = jnp.sum(terms, axis=-1, keepdims=True)
                acc = jnp.dot(
                    terms.astype(jnp.bfloat16),
                    kv_all[keys, 2 * HD : 4 * HD],
                    preferred_element_type=jnp.float32,
                )
                if not first:
                    fade = jnp.exp(last - peak)
                    total = total + fade * totals[m, rows, 0:1]
                    acc = acc + fade * sums[m, rows, :]
                peaks[m, rows, :] = jnp.broadcast_to(peak, (tok, HD))
                totals[m, rows, :] = jnp.broadcast_to(total, (tok, HD))
                sums[m, rows, :] = acc

    attend(z, True)
    for d in range(1, planes):
        here = keys_of((z + planes - d) % planes)

        @pl.when(z - d >= 0)
        def _():
            remote(here, here, kv_send.at[d], kv_recv.at[d], below, tp).wait_recv()

            @pl.when(z + 1 < planes)
            def _():
                remote(here, here, kv_send.at[d + 1], kv_recv.at[d + 1], above, tp).start()

        if d < planes - 1:
            send_weights(planes - 1 - d)
        elif planes == 2:
            send_weights(1)

        @pl.when(z - d >= 0)
        def _():
            attend((z + planes - d) % planes, False)

        if d == 1 and planes > 2:
            share_weights(planes - 1)

    @pl.loop(0, plane)
    def _(chunk):
        rows = block_of(chunk, tok)
        mixed = (
            sums[0, rows, :] / totals[0, rows, 0:1]
            - mix_weight[p] * sums[1, rows, :] / totals[1, rows, 0:1]
        )
        scale = lax.rsqrt(jnp.mean(mixed * mixed, axis=-1, keepdims=True) + epsilon)
        head_out[rows, :] = (mixed * scale * head_gain[...]).astype(jnp.bfloat16)

    own = pltpu.make_async_copy(head_out.at[block_of(p, tok), :], heads.at[p], b_own)
    own.start()
    for d in range(1, plane):
        there = (p + d) % plane
        copy = remote(
            head_out.at[block_of(there, tok), :], heads.at[p],
            b_send.at[d], b_recv.at[d], z * plane + there, tp,
        )
        copy.start()
        started.append(copy)
    own.wait()
    for d in range(1, plane):
        there = (p + plane - d) % plane
        remote(
            heads.at[there], heads.at[there], b_send.at[d], b_recv.at[d], z * plane + there, tp
        ).wait_recv()

    columns = 512

    def product(which, at):
        total = None
        for h in range(plane):
            term = jnp.dot(
                heads[h, block_of(which, half), :],
                out_weight[h * val : (h + 1) * val, at : at + columns],
                preferred_element_type=jnp.float32,
            )
            total = term if total is None else total + term
        return total.astype(jnp.bfloat16)

    model = out_weight.shape[1]
    for at in range(0, model, columns):
        part[:, at : at + columns] = product(other, at)
    swap = remote(part, part_in, t_send, t_recv, sp, other)
    swap.start()
    started.append(swap)
    for at in range(0, model, columns):
        stream[:, at : at + columns] = product(tp, at).astype(jnp.float32)
    swap.wait_recv()
    whole = residual[...].astype(jnp.float32) + (stream[...] + part_in[...].astype(jnp.float32))
    stream[...] = whole
    scaled = whole * lax.rsqrt(jnp.mean(whole * whole, axis=-1, keepdims=True) + epsilon) * gain[...]
    normed[z, block_of(tp, half), :] = scaled.astype(jnp.bfloat16)
    tail[...] = scaled[half - 8 :, :].astype(jnp.bfloat16)

    def tokens(index, which):
        return normed.at[index % planes, block_of(which, half), :]

    mine = tokens(z, tp)

    @pl.when(z + 1 < planes)
    def _():
        remote(mine, mine, up_send.at[1], up_recv.at[1], above, tp).start()

    @pl.when(z > 0)
    def _():
        remote(mine, mine, down_send.at[1], down_recv.at[1], below, tp).start()

    remote(mine, mine, f_send.at[0], f_recv.at[0], sp, other).start()
    after = (p + 1) % plane
    zone = z + (p + 1) // plane

    @pl.when(jnp.logical_and(tp == 1, zone < planes))
    def _():
        for s in range(planes):
            for t in range(2):
                remote(
                    tail, halo.at[zone], h_send.at[s, t], h_recv.at[zone], s * plane + after, t
                ).start()

    for d in range(1, planes):

        @pl.when(z - d >= 0)
        def _():
            theirs = tokens(z + planes - d, tp)
            remote(theirs, theirs, up_send.at[d], up_recv.at[d], below, tp).wait_recv()

            @pl.when(z + 1 < planes)
            def _():
                remote(theirs, theirs, up_send.at[d + 1], up_recv.at[d + 1], above, tp).start()

            remote(theirs, theirs, f_send.at[d], f_recv.at[d], sp, other).start()

        @pl.when(z + d < planes)
        def _():
            theirs = tokens(z + d, tp)
            remote(theirs, theirs, down_send.at[d], down_recv.at[d], above, tp).wait_recv()

            @pl.when(z > 0)
            def _():
                remote(theirs, theirs, down_send.at[d + 1], down_recv.at[d + 1], below, tp).start()

            at = planes - d
            remote(theirs, theirs, f_send.at[at], f_recv.at[at], sp, other).start()

        if d < planes - 1:
            share_weights(planes - 1 - d)
        elif planes == 2:
            share_weights(1)

    for d in range(planes):
        theirs = tokens(z + planes - d, other)
        remote(theirs, theirs, f_send.at[d], f_recv.at[d], sp, other).wait()
    for s in range(planes):

        @pl.when(s * plane + p > 0)
        def _():
            remote(tail, halo.at[s], h_send.at[s, 0], h_recv.at[s], sp, other).wait_recv()

        @pl.when(s * plane + p == 0)
        def _():
            halo[s] = jnp.zeros(halo.shape[1:], halo.dtype)

    for copy in own_weights:
        copy.wait()
    for d in range(planes):
        for e in range(1, plane):
            there = (p + plane - e) % plane
            rows = block_of((z + planes - d) % planes * plane + there, tok)
            for m, dst in enumerate((lift_all, gate_all)):
                remote(
                    dst.at[rows, :], dst.at[rows, :], g_send.at[d, e, m], g_recv.at[d, e, m],
                    z * plane + there, tp,
                ).wait_recv()

    @pl.when(jnp.logical_and(tp == 1, zone < planes))
    def _():
        for s in range(planes):
            for t in range(2):
                remote(tail, halo.at[0], h_send.at[s, t], h_recv.at[0], sp, other).wait_send()

    for d in range(1, planes):

        @pl.when(jnp.logical_and(z + 1 < planes, z - d + 1 >= 0))
        def _():
            remote(keys_of(z), keys_of(z), kv_send.at[d], kv_recv.at[d], above, tp).wait_send()
            remote(mine, mine, up_send.at[d], up_recv.at[d], above, tp).wait_send()

        @pl.when(jnp.logical_and(z > 0, z + d - 1 < planes))
        def _():
            remote(mine, mine, down_send.at[d], down_recv.at[d], below, tp).wait_send()

    for copy in started:
        copy.wait_send()


def down_kernel(
    plane, planes, starts, hidden, weight, stream, out,
    units, total_buf, part, part_in, own_sem, a_send, a_recv, t_send, t_recv,
):
    sp, tp = lax.axis_index("sp"), lax.axis_index("tp")
    z, p = sp // plane, sp % plane
    other = 1 - tp
    tok = units.shape[1]
    half = tok // 2
    greet([((z + d) % planes * plane + p, tp) for d in range(1, planes)] + [(sp, other)])
    started = []
    own = pltpu.make_async_copy(hidden.at[z], units.at[z], own_sem)
    own.start()
    for d in range(1, planes):
        there = (z + d) % planes
        copy = remote(
            hidden.at[there], units.at[z], a_send.at[d], a_recv.at[d], there * plane + p, tp
        )
        copy.start()
        started.append(copy)
    own.wait()
    for d in range(1, planes):
        there = (z + planes - d) % planes
        remote(
            units.at[there], units.at[there], a_send.at[d], a_recv.at[d], sp, other
        ).wait_recv()
    model = weight.shape[1]
    columns = 256

    def product(which, at):
        total = None
        for s in range(planes):
            term = jnp.dot(
                units[s, block_of(which, half), 0 : starts[s + 1] - starts[s]],
                weight[starts[s] : starts[s + 1], block_of(at, columns)],
                preferred_element_type=jnp.float32,
            )
            total = term if total is None else total + term
        return total.astype(jnp.bfloat16)

    @pl.loop(0, model // columns)
    def _(at):
        part[:, block_of(at, columns)] = product(other, at)

    swap = remote(part, part_in, t_send, t_recv, sp, other)
    swap.start()
    started.append(swap)

    @pl.loop(0, model // columns)
    def _(at):
        here = block_of(at, columns)
        total_buf[:, here] = stream[:, here] + product(tp, at).astype(jnp.float32)

    swap.wait_recv()
    out[...] = (total_buf[...] + part_in[...].astype(jnp.float32)).astype(out.dtype)
    for copy in started:
        copy.wait_send()


def shorter_routes(
    plane, planes,
    query_one, key_one, query_two, key_two, values, mix_weight, head_gain, residual, out_weight,
    norm_gain, lift_weight, gate_weight, conv_taps, down_weight,
):
    bf16, f32 = jnp.bfloat16, jnp.float32
    tok = query_one.shape[0]
    model = residual.shape[1]
    val = 2 * HD
    ff = lift_weight.shape[1]
    tiles = ff // 128
    starts = [s * tiles // planes * 128 for s in range(planes + 1)]
    width = -(-tiles // planes) * 128
    count = planes * plane * tok
    sp = lax.axis_index("sp")
    z, p = sp // plane, sp % plane
    dma = pltpu.SemaphoreType.DMA
    anywhere = pl.BlockSpec(memory_space=pl.ANY)
    local = pl.BlockSpec(memory_space=pltpu.VMEM)
    shape = jax.ShapeDtypeStruct

    span = plane * tok
    pair = dma((planes + 1,))
    lift_all, gate_all, normed, halo, stream = pl.pallas_call(
        functools.partial(front_kernel, plane, planes, width),
        out_shape=(
            shape((count, width), bf16),
            shape((count, width), bf16),
            shape((planes, tok, model), bf16),
            shape((planes, 8, model), bf16),
            shape((tok // 2, model), f32),
        ),
        in_specs=[anywhere] * 7 + [pl.BlockSpec(memory_space=pltpu.SMEM)] + [local] * 4,
        out_specs=(anywhere, anywhere, local, local, local),
        scratch_shapes=[
            pltpu.VMEM((span, 2 * HD), bf16),
            pltpu.VMEM((count, 4 * HD), bf16),
            pltpu.VMEM((2, span, HD), f32),
            pltpu.VMEM((2, span, HD), f32),
            pltpu.VMEM((2, span, val), f32),
            pltpu.VMEM((span, val), bf16),
            pltpu.VMEM((plane, tok, val), bf16),
            pltpu.VMEM((tok // 2, model), bf16),
            pltpu.VMEM((tok // 2, model), bf16),
            pltpu.VMEM((8, model), bf16),
            dma((7,)), dma((plane, 5)), dma((plane, 5)), dma((planes, 2)), dma((planes, 2)),
            pair, pair, dma((planes, plane, 2)), dma((planes, plane, 2)),
            dma, dma((plane,)), dma((plane,)), dma, dma, pair, pair, pair, pair,
            dma((planes,)), dma((planes,)), dma((planes, 2)), dma((planes,)),
        ],
        compiler_params=pltpu.CompilerParams(
            collective_id=0, has_side_effects=True, vmem_limit_bytes=40 << 20
        ),
        name="front",
    )(
        query_one, key_one, query_two, key_two, values, lift_weight, gate_weight, mix_weight,
        head_gain.reshape(1, val), out_weight, residual, norm_gain.reshape(1, model),
    )

    rows = jnp.concatenate([halo, normed], axis=1).reshape(planes * (tok + 8), model)
    lifted = jnp.dot(rows, lift_all, preferred_element_type=f32).astype(bf16)
    gated = jnp.dot(rows, gate_all, preferred_element_type=f32).astype(bf16)
    lifted = lifted.reshape(planes, tok + 8, width)[:, 8:].astype(f32)
    gated = gated.reshape(planes, tok + 8, width).astype(f32)
    taps = lax.dynamic_slice_in_dim(conv_taps, z * tiles // planes * 128, width, 1)
    conv = 0.0
    for index in range(WIDTH):
        at = 8 - (WIDTH - 1) + index
        conv = conv + taps[index] * gated[:, at : at + tok]
    hidden = (jax.nn.silu(conv) * lifted).astype(bf16)

    return pl.pallas_call(
        functools.partial(down_kernel, plane, planes, starts),
        out_shape=shape((tok // 2, model), bf16),
        in_specs=[local] * 3,
        out_specs=local,
        scratch_shapes=[
            pltpu.VMEM((planes, tok, width), bf16),
            pltpu.VMEM((tok // 2, model), f32),
            pltpu.VMEM((tok // 2, model), bf16),
            pltpu.VMEM((tok // 2, model), bf16),
            dma, dma((planes,)), dma((planes,)), dma, dma,
        ],
        compiler_params=pltpu.CompilerParams(
            collective_id=1, has_side_effects=True, vmem_limit_bytes=40 << 20
        ),
        name="down",
    )(hidden, down_weight, stream)


def any_route(*arrays):
    tok, heads, ff = arrays[0].shape[0], arrays[5].shape[0], arrays[10].shape[1]
    devices, groups = lax.axis_size("sp"), lax.axis_size("tp")
    planes = devices // heads
    fits = (
        groups == 2 and heads > 1 and planes > 1 and devices % heads == 0
        and ff % 128 == 0 and tok % 128 == 0 and WIDTH <= 9
        and arrays[10].shape[0] == tok
    )
    if fits:
        return shorter_routes(heads, planes, *arrays)
    return on_device(*arrays)


def solution(mesh):
    return jax.shard_map(
        any_route,
        mesh=mesh,
        in_specs=(
            P("sp", "tp"),
            P("sp", "tp"),
            P("sp", "tp"),
            P("sp", "tp"),
            P("sp", "tp"),
            P("tp"),
            P(),
            P(("sp", "tp"), None),
            P("tp", None),
            P(),
            P("sp", "tp"),
            P("sp", "tp"),
            P(None, "tp"),
            P("tp", None),
        ),
        out_specs=P(("sp", "tp"), None),
        check_vma=False,
    )
```

```python
import functools

import jax
import jax.numpy as jnp
from jax import lax
from jax.experimental import pallas as pl
from jax.experimental.pallas import tpu as pltpu
from jax.sharding import PartitionSpec as P

HD = 128
STRETCH = 64
WIDTH = 3


epsilon = 1e-06
masked_score = -1e30


def passed_along(block, axis, distance):
    devices = range(lax.axis_size(axis))
    route = [(i - distance, i) for i in devices if i - distance in devices]
    return lax.ppermute(block, axis, route)


def update_map(peak, total, acc, queries, keys, vals, visible):
    scores = jnp.einsum("thd,shd->hts", queries, keys, preferred_element_type=jnp.float32) * HD ** (
        -0.5
    )
    scores = jnp.where(visible[None], scores, masked_score)
    new_peak = jnp.maximum(peak, jnp.max(scores, axis=-1))
    weights = jnp.where(visible[None], jnp.exp(scores - new_peak[..., None]), 0.0)
    total = jnp.sum(weights, axis=-1)
    acc = jnp.einsum(
        "hts,she->hte", weights.astype(jnp.bfloat16), vals, preferred_element_type=jnp.float32
    )
    return (new_peak, total, acc)


def on_device(
    query_one,
    key_one,
    query_two,
    key_two,
    values,
    mix_weight,
    head_gain,
    residual,
    out_weight,
    norm_gain,
    lift_weight,
    gate_weight,
    conv_taps,
    down_weight,
):
    tok_local = query_one.shape[0]
    heads_local = mix_weight.shape[0]
    val_width = values.shape[1] // heads_local
    model_width = residual.shape[1]
    offset = lax.axis_index("sp") * tok_local
    q_pos = offset + lax.iota(jnp.int32, tok_local)
    q_one = query_one.reshape(tok_local, heads_local, HD)
    q_two = query_two.reshape(tok_local, heads_local, HD)
    start_peak = jnp.full((heads_local, tok_local), masked_score, jnp.float32)
    start_total = jnp.zeros((heads_local, tok_local), jnp.float32)
    start_acc = jnp.zeros((heads_local, tok_local, val_width), jnp.float32)
    initial = (start_peak, start_total, start_acc, start_peak, start_total, start_acc)
    first_keys = lax.all_gather(key_one, "sp", axis=0, tiled=True)
    second_keys = lax.all_gather(key_two, "sp", axis=0, tiled=True)
    piece_vals = lax.all_gather(values, "sp", axis=0, tiled=True)
    count = first_keys.shape[0]
    k_pos = lax.iota(jnp.int32, count)
    visible = k_pos[None, :] // STRETCH <= q_pos[:, None] // STRETCH
    first_keys = first_keys.reshape(count, heads_local, HD)
    second_keys = second_keys.reshape(count, heads_local, HD)
    piece_vals = piece_vals.reshape(count, heads_local, val_width)
    first = update_map(initial[0], initial[1], initial[2], q_one, first_keys, piece_vals, visible)
    second = update_map(initial[3], initial[4], initial[5], q_two, second_keys, piece_vals, visible)
    state = first + second
    mixed = (
        state[2] / state[1][..., None] - mix_weight[:, None, None] * state[5] / state[4][..., None]
    )
    head_out = (
        mixed * lax.rsqrt(jnp.mean(mixed * mixed, axis=-1, keepdims=True) + epsilon) * head_gain
    ).astype(jnp.bfloat16)
    out_heads = out_weight.reshape(heads_local, val_width, model_width)
    piece = head_out
    attended = lax.psum_scatter(
        jnp.einsum("hte,hed->td", piece, out_heads, preferred_element_type=jnp.float32).astype(
            jnp.bfloat16
        ),
        "tp",
        scatter_dimension=0,
        tiled=True,
    ).astype(jnp.float32)
    stream = residual.astype(jnp.float32) + attended
    normed = (
        stream * lax.rsqrt(jnp.mean(stream * stream, axis=-1, keepdims=True) + epsilon) * norm_gain
    ).astype(jnp.bfloat16)
    whole_rows = lax.all_gather(normed, "tp", axis=0, tiled=True)
    lift_pre = jnp.dot(
        whole_rows,
        lax.all_gather(lift_weight, "sp", axis=0, tiled=True),
        preferred_element_type=jnp.float32,
    )
    gate_pre = jnp.dot(
        whole_rows,
        lax.all_gather(gate_weight, "sp", axis=0, tiled=True),
        preferred_element_type=jnp.float32,
    )
    lifted = lift_pre.astype(jnp.bfloat16)
    gated = gate_pre.astype(jnp.bfloat16)
    prior = passed_along(gated[tok_local - (WIDTH - 1) :], "sp", 1)
    extended = jnp.concatenate([prior, gated], axis=0).astype(jnp.float32)
    conv = conv_taps[0] * extended[0:tok_local]
    for index in range(1, WIDTH):
        conv = conv + conv_taps[index] * extended[index : index + tok_local]
    hidden = (jax.nn.silu(conv) * lifted.astype(jnp.float32)).astype(jnp.bfloat16)
    piece = hidden
    mixer = lax.psum_scatter(
        jnp.dot(piece, down_weight, preferred_element_type=jnp.float32).astype(jnp.bfloat16),
        "tp",
        scatter_dimension=0,
        tiled=True,
    ).astype(jnp.float32)
    return (stream + mixer).astype(jnp.bfloat16)

MESH = pl.DeviceIdType.MESH


def remote(src, dst, send_sem, recv_sem, sp, tp):
    return pltpu.make_async_remote_copy(
        src_ref=src,
        dst_ref=dst,
        send_sem=send_sem,
        recv_sem=recv_sem,
        device_id=(sp, tp),
        device_id_type=MESH,
    )


def greet(peers, count=None):
    barrier = pltpu.get_barrier_semaphore()
    for peer in peers:
        pl.semaphore_signal(barrier, inc=1, device_id=peer, device_id_type=MESH)
    pl.semaphore_wait(barrier, len(peers) if count is None else count)


def block_of(index, size):
    return pl.ds(pl.multiple_of(index * size, size), size)


def front_kernel(
    plane, planes, width, q1, k1, q2, k2, v, lift, gate, mix_weight, head_gain, out_hbm, residual_hbm,
    gain,
    lift_all, gate_all, normed, halo, stream,
    q_all, kv_all, peaks, totals, sums, head_out, heads, part, part_in, tail, out_weight, residual,
    own_sem, a_send, a_recv, w_send, w_recv, kv_send, kv_recv, g_send, g_recv,
    b_own, b_send, b_recv, t_send, t_recv, up_send, up_recv, down_send, down_recv,
    f_send, f_recv, h_send, h_recv,
):
    sp, tp = lax.axis_index("sp"), lax.axis_index("tp")
    z, p = sp // plane, sp % plane
    other = 1 - tp
    tok = q1.shape[0]
    half = tok // 2
    val = 2 * HD
    tiles = lift.shape[1] // 128
    before = (p + plane - 1) % plane
    above, below = (z + 1) % planes * plane + p, (z + planes - 1) % planes * plane + p
    weights = ((lift, lift_all), (gate, gate_all))
    peers = (
        [(z * plane + (p + d) % plane, tp) for d in range(1, plane)]
        + [((z + d) % planes * plane + p, tp) for d in range(1, planes)]
        + [(sp, other)]
    )
    barrier = pltpu.get_barrier_semaphore()
    for peer in peers + [(s * plane + before, 1) for s in range(planes)]:
        pl.semaphore_signal(barrier, inc=1, device_id=peer, device_id_type=MESH)

    def piece(head, row):
        h1, h2 = block_of(head, HD), block_of(head, 2 * HD)
        rows, all_rows = block_of(row % plane, tok), block_of(row, tok)
        return [
            (k1.at[:, h1], kv_all.at[all_rows, 0:HD]),
            (k2.at[:, h1], kv_all.at[all_rows, HD : 2 * HD]),
            (v.at[:, h2], kv_all.at[all_rows, 2 * HD : 4 * HD]),
            (q1.at[:, h1], q_all.at[rows, 0:HD]),
            (q2.at[:, h1], q_all.at[rows, HD : 2 * HD]),
        ]

    def units(index):
        return pl.ds(pl.multiple_of(index * tiles // planes * 128, 128), width)

    started = []
    own = [
        pltpu.make_async_copy(src, dst, own_sem.at[n]) for n, (src, dst) in enumerate(piece(p, sp))
    ]
    own_weights = [
        pltpu.make_async_copy(src.at[:, units(z)], dst.at[block_of(sp, tok), :], own_sem.at[5 + m])
        for m, (src, dst) in enumerate(weights)
    ]
    for copy in own:
        copy.start()
    loads = [
        pltpu.make_async_copy(out_hbm, out_weight, own_sem.at[7]),
        pltpu.make_async_copy(residual_hbm, residual, own_sem.at[8]),
    ]
    pl.semaphore_wait(barrier, len(peers) + 2 * planes * tp)
    for d in range(1, plane):
        there = (p + d) % plane
        for n, (src, dst) in enumerate(piece(there, sp)):
            copy = remote(src, dst, a_send.at[d, n], a_recv.at[d, n], z * plane + there, tp)
            copy.start()
            started.append(copy)

    lanes = {}
    for d in range(1, planes):
        there = (z + d) % planes
        lanes[d] = [
            remote(
                src.at[:, units(there)], dst.at[block_of(sp, tok), :],
                w_send.at[d, m], w_recv.at[d, m], there * plane + p, tp,
            )
            for m, (src, dst) in enumerate(weights)
        ]
        started.extend(lanes[d])

    def send_weights(early):
        for d in range(planes - 1, 0, -1):
            if d == planes - 1:
                if early:
                    for copy in lanes[d]:
                        copy.start()
                continue

            @pl.when((z + d >= planes) if early else (z + d < planes))
            def _():
                for copy in lanes[d]:
                    copy.start()

    def share_weights(d):
        source = (z + planes - d) % planes * plane + p
        rows = block_of(source, tok)
        for m, dst in enumerate((lift_all, gate_all)):
            if d:
                remote(
                    dst.at[rows, :], dst.at[rows, :], w_send.at[d, m], w_recv.at[d, m], source, tp
                ).wait_recv()
            src = dst.at[rows, :] if d else weights[m][0].at[:, units(z)]
            for e in range(1, plane):
                copy = remote(
                    src, dst.at[rows, :], g_send.at[d, e, m], g_recv.at[d, e, m],
                    z * plane + (p + e) % plane, tp,
                )
                copy.start()
                started.append(copy)

    send_weights(True)
    share_weights(0)
    for copy in own_weights + loads:
        copy.start()
    for copy in own:
        copy.wait()
    for d in range(1, plane):
        source = z * plane + (p + plane - d) % plane
        for n, (src, dst) in enumerate(piece(p, source)):
            remote(src, dst, a_send.at[d, n], a_recv.at[d, n], source, tp).wait_recv()

    span = plane * tok

    def keys_of(index):
        return kv_all.at[block_of(index, span), :]

    @pl.when(z + 1 < planes)
    def _():
        remote(keys_of(z), keys_of(z), kv_send.at[1], kv_recv.at[1], above, tp).start()

    def attend(source, first):
        @pl.loop(0, plane)
        def _(chunk):
            rows, keys = block_of(chunk, tok), block_of(source, span)
            for m in range(2):
                scores = lax.dot_general(
                    q_all[rows, m * HD : (m + 1) * HD],
                    kv_all[keys, m * HD : (m + 1) * HD],
                    (((1,), (1,)), ((), ())),
                    preferred_element_type=jnp.float32,
                ) * HD ** (-0.5)
                if first:
                    k_pos = lax.broadcasted_iota(jnp.int32, (tok, span), 1)
                    q_pos = chunk * tok + lax.broadcasted_iota(jnp.int32, (tok, span), 0)
                    visible = lax.div(k_pos, STRETCH) <= lax.div(q_pos, STRETCH)
                    scores = jnp.where(visible, scores, masked_score)
                    peak = jnp.max(scores, axis=-1, keepdims=True)
                    terms = jnp.where(visible, jnp.exp(scores - peak), 0.0)
                else:
                    last = peaks[m, rows, 0:1]
                    peak = jnp.maximum(last, jnp.max(scores, axis=-1, keepdims=True))
                    terms = jnp.exp(scores - peak)
                total = jnp.sum(terms, axis=-1, keepdims=True)
                acc = jnp.dot(
                    terms.astype(jnp.bfloat16),
                    kv_all[keys, 2 * HD : 4 * HD],
                    preferred_element_type=jnp.float32,
                )
                if not first:
                    fade = jnp.exp(last - peak)
                    total = total + fade * totals[m, rows, 0:1]
                    acc = acc + fade * sums[m, rows, :]
                peaks[m, rows, :] = jnp.broadcast_to(peak, (tok, HD))
                totals[m, rows, :] = jnp.broadcast_to(total, (tok, HD))
                sums[m, rows, :] = acc

    attend(z, True)
    for d in range(1, planes):
        here = keys_of((z + planes - d) % planes)

        @pl.when(z - d >= 0)
        def _():
            remote(here, here, kv_send.at[d], kv_recv.at[d], below, tp).wait_recv()

            @pl.when(z + 1 < planes)
            def _():
                remote(here, here, kv_send.at[d + 1], kv_recv.at[d + 1], above, tp).start()

        @pl.when(z - d >= 0)
        def _():
            attend((z + planes - d) % planes, False)

        if d == 1:
            share_weights(planes - 1)

    send_weights(False)

    @pl.loop(0, plane)
    def _(chunk):
        rows = block_of(chunk, tok)
        mixed = (
            sums[0, rows, :] / totals[0, rows, 0:1]
            - mix_weight[p] * sums[1, rows, :] / totals[1, rows, 0:1]
        )
        scale = lax.rsqrt(jnp.mean(mixed * mixed, axis=-1, keepdims=True) + epsilon)
        head_out[rows, :] = (mixed * scale * head_gain[...]).astype(jnp.bfloat16)

    own = pltpu.make_async_copy(head_out.at[block_of(p, tok), :], heads.at[p], b_own)
    own.start()
    for d in range(1, plane):
        there = (p + d) % plane
        copy = remote(
            head_out.at[block_of(there, tok), :], heads.at[p],
            b_send.at[d], b_recv.at[d], z * plane + there, tp,
        )
        copy.start()
        started.append(copy)
    own.wait()
    for d in range(1, plane):
        there = (p + plane - d) % plane
        remote(
            heads.at[there], heads.at[there], b_send.at[d], b_recv.at[d], z * plane + there, tp
        ).wait_recv()

    for copy in loads:
        copy.wait()
    columns = 512

    def product(which, at):
        total = None
        for h in range(plane):
            term = jnp.dot(
                heads[h, block_of(which, half), :],
                out_weight[h * val : (h + 1) * val, at : at + columns],
                preferred_element_type=jnp.float32,
            )
            total = term if total is None else total + term
        return total.astype(jnp.bfloat16)

    model = out_weight.shape[1]
    for at in range(0, model, columns):
        part[:, at : at + columns] = product(other, at)
    swap = remote(part, part_in, t_send, t_recv, sp, other)
    swap.start()
    started.append(swap)
    for at in range(0, model, columns):
        stream[:, at : at + columns] = product(tp, at).astype(jnp.float32)
    swap.wait_recv()
    whole = residual[...].astype(jnp.float32) + (stream[...] + part_in[...].astype(jnp.float32))
    stream[...] = whole
    scaled = whole * lax.rsqrt(jnp.mean(whole * whole, axis=-1, keepdims=True) + epsilon) * gain[...]
    normed[z, block_of(tp, half), :] = scaled.astype(jnp.bfloat16)
    tail[...] = scaled[half - 8 :, :].astype(jnp.bfloat16)

    def tokens(index, which):
        return normed.at[index % planes, block_of(which, half), :]

    mine = tokens(z, tp)

    @pl.when(z + 1 < planes)
    def _():
        remote(mine, mine, up_send.at[1], up_recv.at[1], above, tp).start()

    @pl.when(z > 0)
    def _():
        remote(mine, mine, down_send.at[1], down_recv.at[1], below, tp).start()

    remote(mine, mine, f_send.at[0], f_recv.at[0], sp, other).start()
    after = (p + 1) % plane
    zone = z + (p + 1) // plane

    @pl.when(jnp.logical_and(tp == 1, zone < planes))
    def _():
        for s in range(planes):
            for t in range(2):
                remote(
                    tail, halo.at[zone], h_send.at[s, t], h_recv.at[zone], s * plane + after, t
                ).start()

    for d in range(planes - 2, 0, -1):
        share_weights(d)
    for d in range(1, planes):

        @pl.when(z - d >= 0)
        def _():
            theirs = tokens(z + planes - d, tp)
            remote(theirs, theirs, up_send.at[d], up_recv.at[d], below, tp).wait_recv()

            @pl.when(z + 1 < planes)
            def _():
                remote(theirs, theirs, up_send.at[d + 1], up_recv.at[d + 1], above, tp).start()

            remote(theirs, theirs, f_send.at[d], f_recv.at[d], sp, other).start()

        @pl.when(z + d < planes)
        def _():
            theirs = tokens(z + d, tp)
            remote(theirs, theirs, down_send.at[d], down_recv.at[d], above, tp).wait_recv()

            @pl.when(z > 0)
            def _():
                remote(theirs, theirs, down_send.at[d + 1], down_recv.at[d + 1], below, tp).start()

            at = planes - d
            remote(theirs, theirs, f_send.at[at], f_recv.at[at], sp, other).start()

    for d in range(planes):
        theirs = tokens(z + planes - d, other)
        remote(theirs, theirs, f_send.at[d], f_recv.at[d], sp, other).wait()
    for s in range(planes):

        @pl.when(s * plane + p > 0)
        def _():
            remote(tail, halo.at[s], h_send.at[s, 0], h_recv.at[s], sp, other).wait_recv()

        @pl.when(s * plane + p == 0)
        def _():
            halo[s] = jnp.zeros(halo.shape[1:], halo.dtype)

    for copy in own_weights:
        copy.wait()
    for d in range(planes):
        for e in range(1, plane):
            there = (p + plane - e) % plane
            rows = block_of((z + planes - d) % planes * plane + there, tok)
            for m, dst in enumerate((lift_all, gate_all)):
                remote(
                    dst.at[rows, :], dst.at[rows, :], g_send.at[d, e, m], g_recv.at[d, e, m],
                    z * plane + there, tp,
                ).wait_recv()

    @pl.when(jnp.logical_and(tp == 1, zone < planes))
    def _():
        for s in range(planes):
            for t in range(2):
                remote(tail, halo.at[0], h_send.at[s, t], h_recv.at[0], sp, other).wait_send()

    for d in range(1, planes):

        @pl.when(jnp.logical_and(z + 1 < planes, z - d + 1 >= 0))
        def _():
            remote(keys_of(z), keys_of(z), kv_send.at[d], kv_recv.at[d], above, tp).wait_send()
            remote(mine, mine, up_send.at[d], up_recv.at[d], above, tp).wait_send()

        @pl.when(jnp.logical_and(z > 0, z + d - 1 < planes))
        def _():
            remote(mine, mine, down_send.at[d], down_recv.at[d], below, tp).wait_send()

    for copy in started:
        copy.wait_send()


def down_kernel(
    plane, planes, starts, hidden, weight, stream, out,
    held, units, total, part, part_in, l_sem, own_sem, a_send, a_recv, t_send, t_recv,
):
    sp, tp = lax.axis_index("sp"), lax.axis_index("tp")
    z, p = sp // plane, sp % plane
    other = 1 - tp
    tok, width = units.shape[1:]
    half = tok // 2
    tiles = weight.shape[0] // 128

    def load(d):
        at = (z + planes - d) % planes
        first = pl.multiple_of(at * tiles // planes * 128, 128)
        return pltpu.make_async_copy(weight.at[pl.ds(first, width), :], held.at[d], l_sem.at[d])

    for d in range(planes):
        load(d).start()
    greet([((z + d) % planes * plane + p, tp) for d in range(1, planes)] + [(sp, other)])
    started = []
    own = pltpu.make_async_copy(hidden.at[z], units.at[z], own_sem)
    own.start()
    for d in range(1, planes):
        there = (z + d) % planes
        copy = remote(
            hidden.at[there], units.at[z], a_send.at[d], a_recv.at[d], there * plane + p, tp
        )
        copy.start()
        started.append(copy)
    columns = 512
    order = [0] + list(range(1, planes))
    for d in order:
        there = (z + planes - d) % planes
        load(d).wait()
        if d:
            remote(
                units.at[there], units.at[there], a_send.at[d], a_recv.at[d], sp, other
            ).wait_recv()
        else:
            own.wait()

        @pl.loop(0, weight.shape[1] // columns)
        def _(at):
            here = block_of(at, columns)
            term = jnp.dot(units[there], held[d, :, here], preferred_element_type=jnp.float32)
            total[:, here] = term if d == 0 else total[:, here] + term

    part[...] = total[block_of(other, half), :].astype(jnp.bfloat16)
    swap = remote(part, part_in, t_send, t_recv, sp, other)
    swap.start()
    started.append(swap)
    mine = total[block_of(tp, half), :].astype(jnp.bfloat16).astype(jnp.float32)
    swap.wait_recv()
    out[...] = (stream[...] + (mine + part_in[...].astype(jnp.float32))).astype(out.dtype)
    for copy in started:
        copy.wait_send()


def shorter_routes(
    plane, planes,
    query_one, key_one, query_two, key_two, values, mix_weight, head_gain, residual, out_weight,
    norm_gain, lift_weight, gate_weight, conv_taps, down_weight,
):
    bf16, f32 = jnp.bfloat16, jnp.float32
    tok = query_one.shape[0]
    model = residual.shape[1]
    val = 2 * HD
    ff = lift_weight.shape[1]
    tiles = ff // 128
    starts = [s * tiles // planes * 128 for s in range(planes + 1)]
    width = -(-tiles // planes) * 128
    count = planes * plane * tok
    sp = lax.axis_index("sp")
    z, p = sp // plane, sp % plane
    dma = pltpu.SemaphoreType.DMA
    anywhere = pl.BlockSpec(memory_space=pl.ANY)
    local = pl.BlockSpec(memory_space=pltpu.VMEM)
    shape = jax.ShapeDtypeStruct

    span = plane * tok
    pair = dma((planes + 1,))
    lift_all, gate_all, normed, halo, stream = pl.pallas_call(
        functools.partial(front_kernel, plane, planes, width),
        out_shape=(
            shape((count, width), bf16),
            shape((count, width), bf16),
            shape((planes, tok, model), bf16),
            shape((planes, 8, model), bf16),
            shape((tok // 2, model), f32),
        ),
        in_specs=[anywhere] * 7 + [pl.BlockSpec(memory_space=pltpu.SMEM)] + [local, anywhere, anywhere, local],
        out_specs=(anywhere, anywhere, local, local, local),
        scratch_shapes=[
            pltpu.VMEM((span, 2 * HD), bf16),
            pltpu.VMEM((count, 4 * HD), bf16),
            pltpu.VMEM((2, span, HD), f32),
            pltpu.VMEM((2, span, HD), f32),
            pltpu.VMEM((2, span, val), f32),
            pltpu.VMEM((span, val), bf16),
            pltpu.VMEM((plane, tok, val), bf16),
            pltpu.VMEM((tok // 2, model), bf16),
            pltpu.VMEM((tok // 2, model), bf16),
            pltpu.VMEM((8, model), bf16),
            pltpu.VMEM(out_weight.shape, bf16),
            pltpu.VMEM(residual.shape, bf16),
            dma((9,)), dma((plane, 5)), dma((plane, 5)), dma((planes, 2)), dma((planes, 2)),
            pair, pair, dma((planes, plane, 2)), dma((planes, plane, 2)),
            dma, dma((plane,)), dma((plane,)), dma, dma, pair, pair, pair, pair,
            dma((planes,)), dma((planes,)), dma((planes, 2)), dma((planes,)),
        ],
        compiler_params=pltpu.CompilerParams(
            collective_id=0, has_side_effects=True, vmem_limit_bytes=62 << 20
        ),
        name="front",
    )(
        query_one, key_one, query_two, key_two, values, lift_weight, gate_weight, mix_weight,
        head_gain.reshape(1, val), out_weight, residual, norm_gain.reshape(1, model),
    )

    rows = jnp.concatenate([halo, normed], axis=1).reshape(planes * (tok + 8), model)
    lifted = jnp.dot(rows, lift_all, preferred_element_type=f32).astype(bf16)
    gated = jnp.dot(rows, gate_all, preferred_element_type=f32).astype(bf16)
    lifted = lifted.reshape(planes, tok + 8, width)[:, 8:].astype(f32)
    gated = gated.reshape(planes, tok + 8, width).astype(f32)
    taps = lax.dynamic_slice_in_dim(conv_taps, z * tiles // planes * 128, width, 1)
    conv = 0.0
    for index in range(WIDTH):
        at = 8 - (WIDTH - 1) + index
        conv = conv + taps[index] * gated[:, at : at + tok]
    hidden = (jax.nn.silu(conv) * lifted).astype(bf16)
    mine = (z + 1) * tiles // planes * 128 - z * tiles // planes * 128
    hidden = jnp.where(lax.iota(jnp.int32, width) < mine, hidden, 0)

    return pl.pallas_call(
        functools.partial(down_kernel, plane, planes, starts),
        out_shape=shape((tok // 2, model), bf16),
        in_specs=[local, anywhere, local],
        out_specs=local,
        scratch_shapes=[
            pltpu.VMEM((planes, width, model), bf16),
            pltpu.VMEM((planes, tok, width), bf16),
            pltpu.VMEM((tok, model), f32),
            pltpu.VMEM((tok // 2, model), bf16),
            pltpu.VMEM((tok // 2, model), bf16),
            dma((planes,)), dma, dma((planes,)), dma((planes,)), dma, dma,
        ],
        compiler_params=pltpu.CompilerParams(
            collective_id=1, has_side_effects=True, vmem_limit_bytes=62 << 20
        ),
        name="down",
    )(hidden, down_weight, stream)


def any_route(*arrays):
    tok, heads, ff = arrays[0].shape[0], arrays[5].shape[0], arrays[10].shape[1]
    devices, groups = lax.axis_size("sp"), lax.axis_size("tp")
    planes = devices // heads
    fits = (
        groups == 2 and heads > 1 and planes > 1 and devices % heads == 0
        and ff % 128 == 0 and tok % 128 == 0 and WIDTH <= 9
        and arrays[10].shape[0] == tok
    )
    if fits:
        return shorter_routes(heads, planes, *arrays)
    return on_device(*arrays)


def solution(mesh):
    return jax.shard_map(
        any_route,
        mesh=mesh,
        in_specs=(
            P("sp", "tp"),
            P("sp", "tp"),
            P("sp", "tp"),
            P("sp", "tp"),
            P("sp", "tp"),
            P("tp"),
            P(),
            P(("sp", "tp"), None),
            P("tp", None),
            P(),
            P("sp", "tp"),
            P("sp", "tp"),
            P(None, "tp"),
            P("tp", None),
        ),
        out_specs=P(("sp", "tp"), None),
        check_vma=False,
    )
```

```python
import functools

import jax
import jax.numpy as jnp
from jax import lax
from jax.experimental import pallas as pl
from jax.experimental.pallas import tpu as pltpu
from jax.sharding import PartitionSpec as P

HD = 128
STRETCH = 64
WIDTH = 3


epsilon = 1e-06
masked_score = -1e30


def passed_along(block, axis, distance):
    devices = range(lax.axis_size(axis))
    route = [(i - distance, i) for i in devices if i - distance in devices]
    return lax.ppermute(block, axis, route)


def update_map(peak, total, acc, queries, keys, vals, visible):
    scores = jnp.einsum("thd,shd->hts", queries, keys, preferred_element_type=jnp.float32) * HD ** (
        -0.5
    )
    scores = jnp.where(visible[None], scores, masked_score)
    new_peak = jnp.maximum(peak, jnp.max(scores, axis=-1))
    weights = jnp.where(visible[None], jnp.exp(scores - new_peak[..., None]), 0.0)
    total = jnp.sum(weights, axis=-1)
    acc = jnp.einsum(
        "hts,she->hte", weights.astype(jnp.bfloat16), vals, preferred_element_type=jnp.float32
    )
    return (new_peak, total, acc)


def on_device(
    query_one,
    key_one,
    query_two,
    key_two,
    values,
    mix_weight,
    head_gain,
    residual,
    out_weight,
    norm_gain,
    lift_weight,
    gate_weight,
    conv_taps,
    down_weight,
):
    tok_local = query_one.shape[0]
    heads_local = mix_weight.shape[0]
    val_width = values.shape[1] // heads_local
    model_width = residual.shape[1]
    offset = lax.axis_index("sp") * tok_local
    q_pos = offset + lax.iota(jnp.int32, tok_local)
    q_one = query_one.reshape(tok_local, heads_local, HD)
    q_two = query_two.reshape(tok_local, heads_local, HD)
    start_peak = jnp.full((heads_local, tok_local), masked_score, jnp.float32)
    start_total = jnp.zeros((heads_local, tok_local), jnp.float32)
    start_acc = jnp.zeros((heads_local, tok_local, val_width), jnp.float32)
    initial = (start_peak, start_total, start_acc, start_peak, start_total, start_acc)
    first_keys = lax.all_gather(key_one, "sp", axis=0, tiled=True)
    second_keys = lax.all_gather(key_two, "sp", axis=0, tiled=True)
    piece_vals = lax.all_gather(values, "sp", axis=0, tiled=True)
    count = first_keys.shape[0]
    k_pos = lax.iota(jnp.int32, count)
    visible = k_pos[None, :] // STRETCH <= q_pos[:, None] // STRETCH
    first_keys = first_keys.reshape(count, heads_local, HD)
    second_keys = second_keys.reshape(count, heads_local, HD)
    piece_vals = piece_vals.reshape(count, heads_local, val_width)
    first = update_map(initial[0], initial[1], initial[2], q_one, first_keys, piece_vals, visible)
    second = update_map(initial[3], initial[4], initial[5], q_two, second_keys, piece_vals, visible)
    state = first + second
    mixed = (
        state[2] / state[1][..., None] - mix_weight[:, None, None] * state[5] / state[4][..., None]
    )
    head_out = (
        mixed * lax.rsqrt(jnp.mean(mixed * mixed, axis=-1, keepdims=True) + epsilon) * head_gain
    ).astype(jnp.bfloat16)
    out_heads = out_weight.reshape(heads_local, val_width, model_width)
    piece = head_out
    attended = lax.psum_scatter(
        jnp.einsum("hte,hed->td", piece, out_heads, preferred_element_type=jnp.float32).astype(
            jnp.bfloat16
        ),
        "tp",
        scatter_dimension=0,
        tiled=True,
    ).astype(jnp.float32)
    stream = residual.astype(jnp.float32) + attended
    normed = (
        stream * lax.rsqrt(jnp.mean(stream * stream, axis=-1, keepdims=True) + epsilon) * norm_gain
    ).astype(jnp.bfloat16)
    whole_rows = lax.all_gather(normed, "tp", axis=0, tiled=True)
    lift_pre = jnp.dot(
        whole_rows,
        lax.all_gather(lift_weight, "sp", axis=0, tiled=True),
        preferred_element_type=jnp.float32,
    )
    gate_pre = jnp.dot(
        whole_rows,
        lax.all_gather(gate_weight, "sp", axis=0, tiled=True),
        preferred_element_type=jnp.float32,
    )
    lifted = lift_pre.astype(jnp.bfloat16)
    gated = gate_pre.astype(jnp.bfloat16)
    prior = passed_along(gated[tok_local - (WIDTH - 1) :], "sp", 1)
    extended = jnp.concatenate([prior, gated], axis=0).astype(jnp.float32)
    conv = conv_taps[0] * extended[0:tok_local]
    for index in range(1, WIDTH):
        conv = conv + conv_taps[index] * extended[index : index + tok_local]
    hidden = (jax.nn.silu(conv) * lifted.astype(jnp.float32)).astype(jnp.bfloat16)
    piece = hidden
    mixer = lax.psum_scatter(
        jnp.dot(piece, down_weight, preferred_element_type=jnp.float32).astype(jnp.bfloat16),
        "tp",
        scatter_dimension=0,
        tiled=True,
    ).astype(jnp.float32)
    return (stream + mixer).astype(jnp.bfloat16)

MESH = pl.DeviceIdType.MESH


def remote(src, dst, send_sem, recv_sem, sp, tp):
    return pltpu.make_async_remote_copy(
        src_ref=src,
        dst_ref=dst,
        send_sem=send_sem,
        recv_sem=recv_sem,
        device_id=(sp, tp),
        device_id_type=MESH,
    )


def greet(peers, count=None):
    barrier = pltpu.get_barrier_semaphore()
    for peer in peers:
        pl.semaphore_signal(barrier, inc=1, device_id=peer, device_id_type=MESH)
    pl.semaphore_wait(barrier, len(peers) if count is None else count)


def block_of(index, size):
    return pl.ds(pl.multiple_of(index * size, size), size)


def front_kernel(
    plane, planes, width, q1, k1, q2, k2, v, lift, gate, mix_weight, head_gain, out_hbm, residual_hbm,
    gain,
    lift_all, gate_all, normed, halo, stream,
    q_all, kv_all, peaks, totals, sums, head_out, heads, part, part_in, tail, out_weight, residual,
    own_sem, a_send, a_recv, w_send, w_recv, kv_send, kv_recv, g_send, g_recv,
    b_own, b_send, b_recv, t_send, t_recv, up_send, up_recv, down_send, down_recv,
    f_send, f_recv, h_send, h_recv,
):
    sp, tp = lax.axis_index("sp"), lax.axis_index("tp")
    z, p = sp // plane, sp % plane
    other = 1 - tp
    tok = q1.shape[0]
    half = tok // 2
    val = 2 * HD
    tiles = lift.shape[1] // 128
    before = (p + plane - 1) % plane
    above, below = (z + 1) % planes * plane + p, (z + planes - 1) % planes * plane + p
    weights = ((lift, lift_all), (gate, gate_all))
    peers = (
        [(z * plane + (p + d) % plane, tp) for d in range(1, plane)]
        + [((z + d) % planes * plane + p, tp) for d in range(1, planes)]
        + [(sp, other)]
    )
    barrier = pltpu.get_barrier_semaphore()
    for peer in peers + [(s * plane + before, 1) for s in range(planes)]:
        pl.semaphore_signal(barrier, inc=1, device_id=peer, device_id_type=MESH)

    def piece(head, row):
        h1, h2 = block_of(head, HD), block_of(head, 2 * HD)
        rows, all_rows = block_of(row % plane, tok), block_of(row, tok)
        return [
            (k1.at[:, h1], kv_all.at[all_rows, 0:HD]),
            (k2.at[:, h1], kv_all.at[all_rows, HD : 2 * HD]),
            (v.at[:, h2], kv_all.at[all_rows, 2 * HD : 4 * HD]),
            (q1.at[:, h1], q_all.at[rows, 0:HD]),
            (q2.at[:, h1], q_all.at[rows, HD : 2 * HD]),
        ]

    def units(index):
        return pl.ds(pl.multiple_of(index * tiles // planes * 128, 128), width)

    started = []
    own = [
        pltpu.make_async_copy(src, dst, own_sem.at[n]) for n, (src, dst) in enumerate(piece(p, sp))
    ]
    own_weights = [
        pltpu.make_async_copy(src.at[:, units(z)], dst.at[block_of(sp, tok), :], own_sem.at[5 + m])
        for m, (src, dst) in enumerate(weights)
    ]
    for copy in own:
        copy.start()
    loads = [
        pltpu.make_async_copy(out_hbm, out_weight, own_sem.at[7]),
        pltpu.make_async_copy(residual_hbm, residual, own_sem.at[8]),
    ]
    pl.semaphore_wait(barrier, len(peers) + 2 * planes * tp)
    for part_of in ((0, 1, 2), (3, 4)):
        for d in range(1, plane):
            there = (p + d) % plane
            pairs = piece(there, sp)
            for n in part_of:
                src, dst = pairs[n]
                copy = remote(src, dst, a_send.at[d, n], a_recv.at[d, n], z * plane + there, tp)
                copy.start()
                started.append(copy)

    lanes = {}
    for d in range(1, planes):
        there = (z + d) % planes
        lanes[d] = [
            remote(
                src.at[:, units(there)], dst.at[block_of(sp, tok), :],
                w_send.at[d, m], w_recv.at[d, m], there * plane + p, tp,
            )
            for m, (src, dst) in enumerate(weights)
        ]
        started.extend(lanes[d])

    def send_weights(early):
        for d in range(planes - 1, 0, -1):

            @pl.when((z + d >= planes) if early else (z + d < planes))
            def _():
                for copy in lanes[d]:
                    copy.start()

    square = plane == 4
    direct = (1, 2) if square else range(1, plane)

    def partner(e):
        if not square:
            return (p + e) % plane
        flips = {1: p + 1 - 2 * (p % 2), 2: (p + 2) % 4, 3: 3 - p}
        return flips[e]

    def share_weights(d):
        source = (z + planes - d) % planes * plane + p
        rows = block_of(source, tok)
        for m, dst in enumerate((lift_all, gate_all)):
            if d:
                remote(
                    dst.at[rows, :], dst.at[rows, :], w_send.at[d, m], w_recv.at[d, m], source, tp
                ).wait_recv()
            src = dst.at[rows, :] if d else weights[m][0].at[:, units(z)]
            for e in direct:
                copy = remote(
                    src, dst.at[rows, :], g_send.at[d, e, m], g_recv.at[d, e, m],
                    z * plane + partner(e), tp,
                )
                copy.start()
                started.append(copy)

    def pass_weights(d):
        for m, dst in enumerate((lift_all, gate_all)):
            for e in direct:
                there = partner(e) if square else (p + plane - e) % plane
                rows = block_of((z + planes - d) % planes * plane + there, tok)
                block = dst.at[rows, :]
                remote(
                    block, block, g_send.at[d, e, m], g_recv.at[d, e, m], z * plane + there, tp
                ).wait_recv()
                if square and e == m + 1:
                    copy = remote(
                        block, block, g_send.at[d, 3, m], g_recv.at[d, 3, m],
                        z * plane + partner(3 - e), tp,
                    )
                    copy.start()
                    started.append(copy)

    send_weights(True)
    share_weights(0)
    for copy in own_weights + loads:
        copy.start()
    span = plane * tok

    def keys_of(index, e):
        return kv_all.at[block_of(index * plane + (p + plane - e) % plane, tok), :]

    def arrival(e, which):
        source = z * plane + (p + plane - e) % plane
        pairs = piece(p, source)
        for n in which:
            src, dst = pairs[n]
            remote(src, dst, a_send.at[e, n], a_recv.at[e, n], source, tp).wait_recv()

    for e in range(plane):
        if e:
            arrival(e, (0, 1, 2))
        else:
            for copy in own[:3]:
                copy.wait()

        @pl.when(z + 1 < planes)
        def _():
            block = keys_of(z, e)
            remote(block, block, kv_send.at[1, e], kv_recv.at[1, e], above, tp).start()

    for copy in own[3:]:
        copy.wait()
    for e in range(1, plane):
        arrival(e, (3, 4))

    def attend(source, first):
        @pl.loop(0, plane)
        def _(chunk):
            rows, keys = block_of(chunk, tok), block_of(source, span)
            for m in range(2):
                scores = lax.dot_general(
                    q_all[rows, m * HD : (m + 1) * HD],
                    kv_all[keys, m * HD : (m + 1) * HD],
                    (((1,), (1,)), ((), ())),
                    preferred_element_type=jnp.float32,
                ) * HD ** (-0.5)
                if first:
                    k_pos = lax.broadcasted_iota(jnp.int32, (tok, span), 1)
                    q_pos = chunk * tok + lax.broadcasted_iota(jnp.int32, (tok, span), 0)
                    visible = lax.div(k_pos, STRETCH) <= lax.div(q_pos, STRETCH)
                    scores = jnp.where(visible, scores, masked_score)
                    peak = jnp.max(scores, axis=-1, keepdims=True)
                    terms = jnp.where(visible, jnp.exp(scores - peak), 0.0)
                else:
                    last = peaks[m, rows, 0:1]
                    peak = jnp.maximum(last, jnp.max(scores, axis=-1, keepdims=True))
                    terms = jnp.exp(scores - peak)
                total = jnp.sum(terms, axis=-1, keepdims=True)
                acc = jnp.dot(
                    terms.astype(jnp.bfloat16),
                    kv_all[keys, 2 * HD : 4 * HD],
                    preferred_element_type=jnp.float32,
                )
                if not first:
                    fade = jnp.exp(last - peak)
                    total = total + fade * totals[m, rows, 0:1]
                    acc = acc + fade * sums[m, rows, :]
                peaks[m, rows, :] = jnp.broadcast_to(peak, (tok, HD))
                totals[m, rows, :] = jnp.broadcast_to(total, (tok, HD))
                sums[m, rows, :] = acc

    attend(z, True)
    for d in range(1, planes):

        @pl.when(z - d >= 0)
        def _():
            for e in range(plane):
                here = keys_of((z + planes - d) % planes, e)
                remote(here, here, kv_send.at[d, e], kv_recv.at[d, e], below, tp).wait_recv()

                @pl.when(z + 1 < planes)
                def _():
                    remote(
                        here, here, kv_send.at[d + 1, e], kv_recv.at[d + 1, e], above, tp
                    ).start()

        @pl.when(z - d >= 0)
        def _():
            attend((z + planes - d) % planes, False)

        if d == 1:
            pass_weights(0)

    send_weights(False)

    @pl.loop(0, plane)
    def _(chunk):
        rows = block_of(chunk, tok)
        mixed = (
            sums[0, rows, :] / totals[0, rows, 0:1]
            - mix_weight[p] * sums[1, rows, :] / totals[1, rows, 0:1]
        )
        scale = lax.rsqrt(jnp.mean(mixed * mixed, axis=-1, keepdims=True) + epsilon)
        head_out[rows, :] = (mixed * scale * head_gain[...]).astype(jnp.bfloat16)

    own = pltpu.make_async_copy(head_out.at[block_of(p, tok), :], heads.at[p], b_own)
    own.start()
    for d in range(1, plane):
        there = (p + d) % plane
        copy = remote(
            head_out.at[block_of(there, tok), :], heads.at[p],
            b_send.at[d], b_recv.at[d], z * plane + there, tp,
        )
        copy.start()
        started.append(copy)
    own.wait()
    share_weights(planes - 1)
    for d in range(1, plane):
        there = (p + plane - d) % plane
        remote(
            heads.at[there], heads.at[there], b_send.at[d], b_recv.at[d], z * plane + there, tp
        ).wait_recv()

    for copy in loads:
        copy.wait()
    columns = 512

    def product(which, at):
        total = None
        for h in range(plane):
            term = jnp.dot(
                heads[h, block_of(which, half), :],
                out_weight[h * val : (h + 1) * val, at : at + columns],
                preferred_element_type=jnp.float32,
            )
            total = term if total is None else total + term
        return total.astype(jnp.bfloat16)

    model = out_weight.shape[1]
    for at in range(0, model, columns):
        part[:, at : at + columns] = product(other, at)
    swap = remote(part, part_in, t_send, t_recv, sp, other)
    swap.start()
    started.append(swap)
    for at in range(0, model, columns):
        stream[:, at : at + columns] = product(tp, at).astype(jnp.float32)
    swap.wait_recv()
    whole = residual[...].astype(jnp.float32) + (stream[...] + part_in[...].astype(jnp.float32))
    stream[...] = whole
    scaled = whole * lax.rsqrt(jnp.mean(whole * whole, axis=-1, keepdims=True) + epsilon) * gain[...]
    normed[z, block_of(tp, half), :] = scaled.astype(jnp.bfloat16)
    tail[...] = scaled[half - 8 :, :].astype(jnp.bfloat16)

    def tokens(index, which):
        return normed.at[index % planes, block_of(which, half), :]

    mine = tokens(z, tp)

    @pl.when(z + 1 < planes)
    def _():
        remote(mine, mine, up_send.at[1], up_recv.at[1], above, tp).start()

    @pl.when(z > 0)
    def _():
        remote(mine, mine, down_send.at[1], down_recv.at[1], below, tp).start()

    remote(mine, mine, f_send.at[0], f_recv.at[0], sp, other).start()
    after = (p + 1) % plane
    zone = z + (p + 1) // plane

    @pl.when(jnp.logical_and(tp == 1, zone < planes))
    def _():
        for s in range(planes):
            for t in range(2):
                remote(
                    tail, halo.at[zone], h_send.at[s, t], h_recv.at[zone], s * plane + after, t
                ).start()

    for d in range(planes - 2, 0, -1):
        share_weights(d)
        pass_weights(d + 1)
    for d in range(1, planes):

        @pl.when(z - d >= 0)
        def _():
            theirs = tokens(z + planes - d, tp)
            remote(theirs, theirs, up_send.at[d], up_recv.at[d], below, tp).wait_recv()

            @pl.when(z + 1 < planes)
            def _():
                remote(theirs, theirs, up_send.at[d + 1], up_recv.at[d + 1], above, tp).start()

            remote(theirs, theirs, f_send.at[d], f_recv.at[d], sp, other).start()

        @pl.when(z + d < planes)
        def _():
            theirs = tokens(z + d, tp)
            remote(theirs, theirs, down_send.at[d], down_recv.at[d], above, tp).wait_recv()

            @pl.when(z > 0)
            def _():
                remote(theirs, theirs, down_send.at[d + 1], down_recv.at[d + 1], below, tp).start()

            at = planes - d
            remote(theirs, theirs, f_send.at[at], f_recv.at[at], sp, other).start()

    for d in range(planes):
        theirs = tokens(z + planes - d, other)
        remote(theirs, theirs, f_send.at[d], f_recv.at[d], sp, other).wait()
    for s in range(planes):

        @pl.when(s * plane + p > 0)
        def _():
            remote(tail, halo.at[s], h_send.at[s, 0], h_recv.at[s], sp, other).wait_recv()

        @pl.when(s * plane + p == 0)
        def _():
            halo[s] = jnp.zeros(halo.shape[1:], halo.dtype)

    pass_weights(1)
    for copy in own_weights:
        copy.wait()
    for d in range(planes):
        for e in (3,) if square else ():
            there = partner(e)
            rows = block_of((z + planes - d) % planes * plane + there, tok)
            for m, dst in enumerate((lift_all, gate_all)):
                remote(
                    dst.at[rows, :], dst.at[rows, :], g_send.at[d, e, m], g_recv.at[d, e, m],
                    z * plane + there, tp,
                ).wait_recv()

    @pl.when(jnp.logical_and(tp == 1, zone < planes))
    def _():
        for s in range(planes):
            for t in range(2):
                remote(tail, halo.at[0], h_send.at[s, t], h_recv.at[0], sp, other).wait_send()

    for d in range(1, planes):

        @pl.when(jnp.logical_and(z + 1 < planes, z - d + 1 >= 0))
        def _():
            for e in range(plane):
                block = keys_of(z, e)
                remote(block, block, kv_send.at[d, e], kv_recv.at[d, e], above, tp).wait_send()
            remote(mine, mine, up_send.at[d], up_recv.at[d], above, tp).wait_send()

        @pl.when(jnp.logical_and(z > 0, z + d - 1 < planes))
        def _():
            remote(mine, mine, down_send.at[d], down_recv.at[d], below, tp).wait_send()

    for copy in started:
        copy.wait_send()


def down_kernel(
    plane, planes, starts, hidden, weight, stream, out,
    held, units, total, part, part_in, l_sem, own_sem, a_send, a_recv, t_send, t_recv,
):
    sp, tp = lax.axis_index("sp"), lax.axis_index("tp")
    z, p = sp // plane, sp % plane
    other = 1 - tp
    tok, width = units.shape[1:]
    half = tok // 2
    tiles = weight.shape[0] // 128

    def load(d):
        at = (z + planes - d) % planes
        first = pl.multiple_of(at * tiles // planes * 128, 128)
        return pltpu.make_async_copy(weight.at[pl.ds(first, width), :], held.at[d], l_sem.at[d])

    for d in range(planes):
        load(d).start()
    greet([((z + d) % planes * plane + p, tp) for d in range(1, planes)] + [(sp, other)])
    started = []
    own = pltpu.make_async_copy(hidden.at[z], units.at[z], own_sem)
    own.start()
    for d in range(1, planes):
        there = (z + d) % planes
        copy = remote(
            hidden.at[there], units.at[z], a_send.at[d], a_recv.at[d], there * plane + p, tp
        )
        copy.start()
        started.append(copy)
    columns = 512
    order = [0] + list(range(1, planes))
    for d in order:
        there = (z + planes - d) % planes
        load(d).wait()
        if d:
            remote(
                units.at[there], units.at[there], a_send.at[d], a_recv.at[d], sp, other
            ).wait_recv()
        else:
            own.wait()

        @pl.loop(0, weight.shape[1] // columns)
        def _(at):
            here = block_of(at, columns)
            term = jnp.dot(units[there], held[d, :, here], preferred_element_type=jnp.float32)
            total[:, here] = term if d == 0 else total[:, here] + term

    part[...] = total[block_of(other, half), :].astype(jnp.bfloat16)
    swap = remote(part, part_in, t_send, t_recv, sp, other)
    swap.start()
    started.append(swap)
    mine = total[block_of(tp, half), :].astype(jnp.bfloat16).astype(jnp.float32)
    swap.wait_recv()
    out[...] = (stream[...] + (mine + part_in[...].astype(jnp.float32))).astype(out.dtype)
    for copy in started:
        copy.wait_send()


def shorter_routes(
    plane, planes,
    query_one, key_one, query_two, key_two, values, mix_weight, head_gain, residual, out_weight,
    norm_gain, lift_weight, gate_weight, conv_taps, down_weight,
):
    bf16, f32 = jnp.bfloat16, jnp.float32
    tok = query_one.shape[0]
    model = residual.shape[1]
    val = 2 * HD
    ff = lift_weight.shape[1]
    tiles = ff // 128
    starts = [s * tiles // planes * 128 for s in range(planes + 1)]
    width = -(-tiles // planes) * 128
    count = planes * plane * tok
    sp = lax.axis_index("sp")
    z, p = sp // plane, sp % plane
    dma = pltpu.SemaphoreType.DMA
    anywhere = pl.BlockSpec(memory_space=pl.ANY)
    local = pl.BlockSpec(memory_space=pltpu.VMEM)
    shape = jax.ShapeDtypeStruct

    span = plane * tok
    pair = dma((planes + 1,))
    lift_all, gate_all, normed, halo, stream = pl.pallas_call(
        functools.partial(front_kernel, plane, planes, width),
        out_shape=(
            shape((count, width), bf16),
            shape((count, width), bf16),
            shape((planes, tok, model), bf16),
            shape((planes, 8, model), bf16),
            shape((tok // 2, model), f32),
        ),
        in_specs=[anywhere] * 7 + [pl.BlockSpec(memory_space=pltpu.SMEM)] + [local, anywhere, anywhere, local],
        out_specs=(anywhere, anywhere, local, local, local),
        scratch_shapes=[
            pltpu.VMEM((span, 2 * HD), bf16),
            pltpu.VMEM((count, 4 * HD), bf16),
            pltpu.VMEM((2, span, HD), f32),
            pltpu.VMEM((2, span, HD), f32),
            pltpu.VMEM((2, span, val), f32),
            pltpu.VMEM((span, val), bf16),
            pltpu.VMEM((plane, tok, val), bf16),
            pltpu.VMEM((tok // 2, model), bf16),
            pltpu.VMEM((tok // 2, model), bf16),
            pltpu.VMEM((8, model), bf16),
            pltpu.VMEM(out_weight.shape, bf16),
            pltpu.VMEM(residual.shape, bf16),
            dma((9,)), dma((plane, 5)), dma((plane, 5)), dma((planes, 2)), dma((planes, 2)),
            dma((planes + 1, plane)), dma((planes + 1, plane)), dma((planes, plane, 2)), dma((planes, plane, 2)),
            dma, dma((plane,)), dma((plane,)), dma, dma, pair, pair, pair, pair,
            dma((planes,)), dma((planes,)), dma((planes, 2)), dma((planes,)),
        ],
        compiler_params=pltpu.CompilerParams(
            collective_id=0, has_side_effects=True, vmem_limit_bytes=62 << 20
        ),
        name="front",
    )(
        query_one, key_one, query_two, key_two, values, lift_weight, gate_weight, mix_weight,
        head_gain.reshape(1, val), out_weight, residual, norm_gain.reshape(1, model),
    )

    rows = jnp.concatenate([halo, normed], axis=1).reshape(planes * (tok + 8), model)
    lifted = jnp.dot(rows, lift_all, preferred_element_type=f32).astype(bf16)
    gated = jnp.dot(rows, gate_all, preferred_element_type=f32).astype(bf16)
    lifted = lifted.reshape(planes, tok + 8, width)[:, 8:].astype(f32)
    gated = gated.reshape(planes, tok + 8, width).astype(f32)
    taps = lax.dynamic_slice_in_dim(conv_taps, z * tiles // planes * 128, width, 1)
    conv = 0.0
    for index in range(WIDTH):
        at = 8 - (WIDTH - 1) + index
        conv = conv + taps[index] * gated[:, at : at + tok]
    hidden = (jax.nn.silu(conv) * lifted).astype(bf16)
    mine = (z + 1) * tiles // planes * 128 - z * tiles // planes * 128
    hidden = jnp.where(lax.iota(jnp.int32, width) < mine, hidden, 0)

    return pl.pallas_call(
        functools.partial(down_kernel, plane, planes, starts),
        out_shape=shape((tok // 2, model), bf16),
        in_specs=[local, anywhere, local],
        out_specs=local,
        scratch_shapes=[
            pltpu.VMEM((planes, width, model), bf16),
            pltpu.VMEM((planes, tok, width), bf16),
            pltpu.VMEM((tok, model), f32),
            pltpu.VMEM((tok // 2, model), bf16),
            pltpu.VMEM((tok // 2, model), bf16),
            dma((planes,)), dma, dma((planes,)), dma((planes,)), dma, dma,
        ],
        compiler_params=pltpu.CompilerParams(
            collective_id=1, has_side_effects=True, vmem_limit_bytes=62 << 20
        ),
        name="down",
    )(hidden, down_weight, stream)


def any_route(*arrays):
    tok, heads, ff = arrays[0].shape[0], arrays[5].shape[0], arrays[10].shape[1]
    devices, groups = lax.axis_size("sp"), lax.axis_size("tp")
    planes = devices // heads
    fits = (
        groups == 2 and heads > 1 and planes > 1 and devices % heads == 0
        and ff % 128 == 0 and tok % 128 == 0 and WIDTH <= 9
        and arrays[10].shape[0] == tok
    )
    if fits:
        return shorter_routes(heads, planes, *arrays)
    return on_device(*arrays)


def solution(mesh):
    return jax.shard_map(
        any_route,
        mesh=mesh,
        in_specs=(
            P("sp", "tp"),
            P("sp", "tp"),
            P("sp", "tp"),
            P("sp", "tp"),
            P("sp", "tp"),
            P("tp"),
            P(),
            P(("sp", "tp"), None),
            P("tp", None),
            P(),
            P("sp", "tp"),
            P("sp", "tp"),
            P(None, "tp"),
            P("tp", None),
        ),
        out_specs=P(("sp", "tp"), None),
        check_vma=False,
    )
```

```python
import functools

import jax
import jax.numpy as jnp
from jax import lax
from jax.experimental import pallas as pl
from jax.experimental.pallas import tpu as pltpu
from jax.sharding import PartitionSpec as P

HD = 128
STRETCH = 64
WIDTH = 3


epsilon = 1e-06
masked_score = -1e30


def passed_along(block, axis, distance):
    devices = range(lax.axis_size(axis))
    route = [(i - distance, i) for i in devices if i - distance in devices]
    return lax.ppermute(block, axis, route)


def update_map(peak, total, acc, queries, keys, vals, visible):
    scores = jnp.einsum("thd,shd->hts", queries, keys, preferred_element_type=jnp.float32) * HD ** (
        -0.5
    )
    scores = jnp.where(visible[None], scores, masked_score)
    new_peak = jnp.maximum(peak, jnp.max(scores, axis=-1))
    weights = jnp.where(visible[None], jnp.exp(scores - new_peak[..., None]), 0.0)
    total = jnp.sum(weights, axis=-1)
    acc = jnp.einsum(
        "hts,she->hte", weights.astype(jnp.bfloat16), vals, preferred_element_type=jnp.float32
    )
    return (new_peak, total, acc)


def on_device(
    query_one,
    key_one,
    query_two,
    key_two,
    values,
    mix_weight,
    head_gain,
    residual,
    out_weight,
    norm_gain,
    lift_weight,
    gate_weight,
    conv_taps,
    down_weight,
):
    tok_local = query_one.shape[0]
    heads_local = mix_weight.shape[0]
    val_width = values.shape[1] // heads_local
    model_width = residual.shape[1]
    offset = lax.axis_index("sp") * tok_local
    q_pos = offset + lax.iota(jnp.int32, tok_local)
    q_one = query_one.reshape(tok_local, heads_local, HD)
    q_two = query_two.reshape(tok_local, heads_local, HD)
    start_peak = jnp.full((heads_local, tok_local), masked_score, jnp.float32)
    start_total = jnp.zeros((heads_local, tok_local), jnp.float32)
    start_acc = jnp.zeros((heads_local, tok_local, val_width), jnp.float32)
    initial = (start_peak, start_total, start_acc, start_peak, start_total, start_acc)
    first_keys = lax.all_gather(key_one, "sp", axis=0, tiled=True)
    second_keys = lax.all_gather(key_two, "sp", axis=0, tiled=True)
    piece_vals = lax.all_gather(values, "sp", axis=0, tiled=True)
    count = first_keys.shape[0]
    k_pos = lax.iota(jnp.int32, count)
    visible = k_pos[None, :] // STRETCH <= q_pos[:, None] // STRETCH
    first_keys = first_keys.reshape(count, heads_local, HD)
    second_keys = second_keys.reshape(count, heads_local, HD)
    piece_vals = piece_vals.reshape(count, heads_local, val_width)
    first = update_map(initial[0], initial[1], initial[2], q_one, first_keys, piece_vals, visible)
    second = update_map(initial[3], initial[4], initial[5], q_two, second_keys, piece_vals, visible)
    state = first + second
    mixed = (
        state[2] / state[1][..., None] - mix_weight[:, None, None] * state[5] / state[4][..., None]
    )
    head_out = (
        mixed * lax.rsqrt(jnp.mean(mixed * mixed, axis=-1, keepdims=True) + epsilon) * head_gain
    ).astype(jnp.bfloat16)
    out_heads = out_weight.reshape(heads_local, val_width, model_width)
    piece = head_out
    attended = lax.psum_scatter(
        jnp.einsum("hte,hed->td", piece, out_heads, preferred_element_type=jnp.float32).astype(
            jnp.bfloat16
        ),
        "tp",
        scatter_dimension=0,
        tiled=True,
    ).astype(jnp.float32)
    stream = residual.astype(jnp.float32) + attended
    normed = (
        stream * lax.rsqrt(jnp.mean(stream * stream, axis=-1, keepdims=True) + epsilon) * norm_gain
    ).astype(jnp.bfloat16)
    whole_rows = lax.all_gather(normed, "tp", axis=0, tiled=True)
    lift_pre = jnp.dot(
        whole_rows,
        lax.all_gather(lift_weight, "sp", axis=0, tiled=True),
        preferred_element_type=jnp.float32,
    )
    gate_pre = jnp.dot(
        whole_rows,
        lax.all_gather(gate_weight, "sp", axis=0, tiled=True),
        preferred_element_type=jnp.float32,
    )
    lifted = lift_pre.astype(jnp.bfloat16)
    gated = gate_pre.astype(jnp.bfloat16)
    prior = passed_along(gated[tok_local - (WIDTH - 1) :], "sp", 1)
    extended = jnp.concatenate([prior, gated], axis=0).astype(jnp.float32)
    conv = conv_taps[0] * extended[0:tok_local]
    for index in range(1, WIDTH):
        conv = conv + conv_taps[index] * extended[index : index + tok_local]
    hidden = (jax.nn.silu(conv) * lifted.astype(jnp.float32)).astype(jnp.bfloat16)
    piece = hidden
    mixer = lax.psum_scatter(
        jnp.dot(piece, down_weight, preferred_element_type=jnp.float32).astype(jnp.bfloat16),
        "tp",
        scatter_dimension=0,
        tiled=True,
    ).astype(jnp.float32)
    return (stream + mixer).astype(jnp.bfloat16)

MESH = pl.DeviceIdType.MESH


def remote(src, dst, send_sem, recv_sem, sp, tp):
    return pltpu.make_async_remote_copy(
        src_ref=src,
        dst_ref=dst,
        send_sem=send_sem,
        recv_sem=recv_sem,
        device_id=(sp, tp),
        device_id_type=MESH,
    )


def greet(peers, count=None):
    barrier = pltpu.get_barrier_semaphore()
    for peer in peers:
        pl.semaphore_signal(barrier, inc=1, device_id=peer, device_id_type=MESH)
    pl.semaphore_wait(barrier, len(peers) if count is None else count)


def block_of(index, size):
    return pl.ds(pl.multiple_of(index * size, size), size)


def front_kernel(
    plane, planes, width, q1, k1, q2, k2, v, lift, gate, mix_weight, head_gain, out_hbm, residual_hbm,
    gain,
    lift_all, gate_all, normed, halo, stream,
    q_all, kv_all, peaks, totals, sums, head_out, heads, part, part_in, tail, out_weight, residual,
    own_sem, a_send, a_recv, w_send, w_recv, kv_send, kv_recv, g_send, g_recv,
    b_own, b_send, b_recv, t_send, t_recv, up_send, up_recv, down_send, down_recv,
    f_send, f_recv, h_send, h_recv,
):
    sp, tp = lax.axis_index("sp"), lax.axis_index("tp")
    z, p = sp // plane, sp % plane
    other = 1 - tp
    tok = q1.shape[0]
    half = tok // 2
    val = 2 * HD
    tiles = lift.shape[1] // 128
    before = (p + plane - 1) % plane
    above, below = (z + 1) % planes * plane + p, (z + planes - 1) % planes * plane + p
    weights = ((lift, lift_all), (gate, gate_all))
    peers = (
        [(z * plane + (p + d) % plane, tp) for d in range(1, plane)]
        + [((z + d) % planes * plane + p, tp) for d in range(1, planes)]
        + [(sp, other)]
    )
    barrier = pltpu.get_barrier_semaphore()
    for peer in peers + [(s * plane + before, 1) for s in range(planes)]:
        pl.semaphore_signal(barrier, inc=1, device_id=peer, device_id_type=MESH)

    def piece(head, row):
        h1, h2 = block_of(head, HD), block_of(head, 2 * HD)
        rows, all_rows = block_of(row % plane, tok), block_of(row, tok)
        return [
            (k1.at[:, h1], kv_all.at[all_rows, 0:HD]),
            (k2.at[:, h1], kv_all.at[all_rows, HD : 2 * HD]),
            (v.at[:, h2], kv_all.at[all_rows, 2 * HD : 4 * HD]),
            (q1.at[:, h1], q_all.at[rows, 0:HD]),
            (q2.at[:, h1], q_all.at[rows, HD : 2 * HD]),
        ]

    def units(index):
        return pl.ds(pl.multiple_of(index * tiles // planes * 128, 128), width)

    started = []
    own = [
        pltpu.make_async_copy(src, dst, own_sem.at[n]) for n, (src, dst) in enumerate(piece(p, sp))
    ]
    own_weights = [
        pltpu.make_async_copy(src.at[:, units(z)], dst.at[block_of(sp, tok), :], own_sem.at[5 + m])
        for m, (src, dst) in enumerate(weights)
    ]
    for copy in own:
        copy.start()
    loads = [
        pltpu.make_async_copy(out_hbm, out_weight, own_sem.at[7]),
        pltpu.make_async_copy(residual_hbm, residual, own_sem.at[8]),
    ]
    pl.semaphore_wait(barrier, len(peers) + 2 * planes * tp)
    for part_of in ((0, 1, 2), (3, 4)):
        for d in range(1, plane):
            there = (p + d) % plane
            pairs = piece(there, sp)
            for n in part_of:
                src, dst = pairs[n]
                copy = remote(src, dst, a_send.at[d, n], a_recv.at[d, n], z * plane + there, tp)
                copy.start()
                started.append(copy)

    lanes = {}
    for d in range(1, planes):
        there = (z + d) % planes
        lanes[d] = [
            remote(
                src.at[:, units(there)], dst.at[block_of(sp, tok), :],
                w_send.at[d, m], w_recv.at[d, m], there * plane + p, tp,
            )
            for m, (src, dst) in enumerate(weights)
        ]
        started.extend(lanes[d])

    def send_weights(early):
        for d in range(planes - 1, 0, -1):

            @pl.when((z + d >= planes) if early else (z + d < planes))
            def _():
                for copy in lanes[d]:
                    copy.start()

    square = plane == 4
    direct = (1, 2) if square else range(1, plane)

    def partner(e):
        if not square:
            return (p + e) % plane
        flips = {1: p + 1 - 2 * (p % 2), 2: (p + 2) % 4, 3: 3 - p}
        return flips[e]

    def share_weights(d, condition=None, record=True):
        source = (z + planes - d) % planes * plane + p
        rows = block_of(source, tok)
        arrivals, copies = [], []
        for m, dst in enumerate((lift_all, gate_all)):
            block = dst.at[rows, :]
            if d:
                arrivals.append(
                    remote(block, block, w_send.at[d, m], w_recv.at[d, m], source, tp)
                )
            src = block if d else weights[m][0].at[:, units(z)]
            copies.append(
                [
                    remote(
                        src, block, g_send.at[d, e, m], g_recv.at[d, e, m],
                        z * plane + partner(e), tp,
                    )
                    for e in direct
                ]
            )

        def run():
            for m in range(2):
                if d:
                    arrivals[m].wait_recv()
                for copy in copies[m]:
                    copy.start()

        if condition is None:
            run()
        else:
            pl.when(condition)(run)
        if record:
            started.extend(copies[0] + copies[1])

    def pass_weights(d):
        for m, dst in enumerate((lift_all, gate_all)):
            for e in direct:
                there = partner(e) if square else (p + plane - e) % plane
                rows = block_of((z + planes - d) % planes * plane + there, tok)
                block = dst.at[rows, :]
                remote(
                    block, block, g_send.at[d, e, m], g_recv.at[d, e, m], z * plane + there, tp
                ).wait_recv()
                if square and e == m + 1:
                    copy = remote(
                        block, block, g_send.at[d, 3, m], g_recv.at[d, 3, m],
                        z * plane + partner(3 - e), tp,
                    )
                    copy.start()
                    started.append(copy)

    send_weights(True)
    share_weights(0)
    for copy in own_weights + loads:
        copy.start()
    span = plane * tok

    def keys_of(index, e):
        return kv_all.at[block_of(index * plane + (p + plane - e) % plane, tok), :]

    def arrival(e, which):
        source = z * plane + (p + plane - e) % plane
        pairs = piece(p, source)
        for n in which:
            src, dst = pairs[n]
            remote(src, dst, a_send.at[e, n], a_recv.at[e, n], source, tp).wait_recv()

    for e in range(plane):
        if e:
            arrival(e, (0, 1, 2))
        else:
            for copy in own[:3]:
                copy.wait()

        @pl.when(z + 1 < planes)
        def _():
            block = keys_of(z, e)
            remote(block, block, kv_send.at[1, e], kv_recv.at[1, e], above, tp).start()

    for copy in own[3:]:
        copy.wait()
    for e in range(1, plane):
        arrival(e, (3, 4))

    def attend(source, first):
        @pl.loop(0, plane)
        def _(chunk):
            rows, keys = block_of(chunk, tok), block_of(source, span)
            for m in range(2):
                scores = lax.dot_general(
                    q_all[rows, m * HD : (m + 1) * HD],
                    kv_all[keys, m * HD : (m + 1) * HD],
                    (((1,), (1,)), ((), ())),
                    preferred_element_type=jnp.float32,
                ) * HD ** (-0.5)
                if first:
                    k_pos = lax.broadcasted_iota(jnp.int32, (tok, span), 1)
                    q_pos = chunk * tok + lax.broadcasted_iota(jnp.int32, (tok, span), 0)
                    visible = lax.div(k_pos, STRETCH) <= lax.div(q_pos, STRETCH)
                    scores = jnp.where(visible, scores, masked_score)
                    peak = jnp.max(scores, axis=-1, keepdims=True)
                    terms = jnp.where(visible, jnp.exp(scores - peak), 0.0)
                else:
                    last = peaks[m, rows, 0:1]
                    peak = jnp.maximum(last, jnp.max(scores, axis=-1, keepdims=True))
                    terms = jnp.exp(scores - peak)
                total = jnp.sum(terms, axis=-1, keepdims=True)
                acc = jnp.dot(
                    terms.astype(jnp.bfloat16),
                    kv_all[keys, 2 * HD : 4 * HD],
                    preferred_element_type=jnp.float32,
                )
                if not first:
                    fade = jnp.exp(last - peak)
                    total = total + fade * totals[m, rows, 0:1]
                    acc = acc + fade * sums[m, rows, :]
                peaks[m, rows, :] = jnp.broadcast_to(peak, (tok, HD))
                totals[m, rows, :] = jnp.broadcast_to(total, (tok, HD))
                sums[m, rows, :] = acc

    attend(z, True)
    for d in range(1, planes):

        @pl.when(z - d >= 0)
        def _():
            for e in range(plane):
                here = keys_of((z + planes - d) % planes, e)
                remote(here, here, kv_send.at[d, e], kv_recv.at[d, e], below, tp).wait_recv()

                @pl.when(z + 1 < planes)
                def _():
                    remote(
                        here, here, kv_send.at[d + 1, e], kv_recv.at[d + 1, e], above, tp
                    ).start()

        @pl.when(z - d >= 0)
        def _():
            attend((z + planes - d) % planes, False)

        if d == 1:
            pass_weights(0)

    send_weights(False)

    @pl.loop(0, plane)
    def _(chunk):
        rows = block_of(chunk, tok)
        mixed = (
            sums[0, rows, :] / totals[0, rows, 0:1]
            - mix_weight[p] * sums[1, rows, :] / totals[1, rows, 0:1]
        )
        scale = lax.rsqrt(jnp.mean(mixed * mixed, axis=-1, keepdims=True) + epsilon)
        head_out[rows, :] = (mixed * scale * head_gain[...]).astype(jnp.bfloat16)

    own = pltpu.make_async_copy(head_out.at[block_of(p, tok), :], heads.at[p], b_own)
    own.start()
    for d in range(1, plane):
        there = (p + d) % plane
        copy = remote(
            head_out.at[block_of(there, tok), :], heads.at[p],
            b_send.at[d], b_recv.at[d], z * plane + there, tp,
        )
        copy.start()
        started.append(copy)
    own.wait()
    share_weights(planes - 1, z < planes - 1)
    for d in range(1, plane):
        there = (p + plane - d) % plane
        remote(
            heads.at[there], heads.at[there], b_send.at[d], b_recv.at[d], z * plane + there, tp
        ).wait_recv()

    for copy in loads:
        copy.wait()
    columns = 512

    def product(which, at):
        total = None
        for h in range(plane):
            term = jnp.dot(
                heads[h, block_of(which, half), :],
                out_weight[h * val : (h + 1) * val, at : at + columns],
                preferred_element_type=jnp.float32,
            )
            total = term if total is None else total + term
        return total.astype(jnp.bfloat16)

    model = out_weight.shape[1]
    for at in range(0, model, columns):
        part[:, at : at + columns] = product(other, at)
    swap = remote(part, part_in, t_send, t_recv, sp, other)
    swap.start()
    started.append(swap)
    for at in range(0, model, columns):
        stream[:, at : at + columns] = product(tp, at).astype(jnp.float32)
    swap.wait_recv()
    whole = residual[...].astype(jnp.float32) + (stream[...] + part_in[...].astype(jnp.float32))
    stream[...] = whole
    scaled = whole * lax.rsqrt(jnp.mean(whole * whole, axis=-1, keepdims=True) + epsilon) * gain[...]
    normed[z, block_of(tp, half), :] = scaled.astype(jnp.bfloat16)
    tail[...] = scaled[half - 8 :, :].astype(jnp.bfloat16)

    def tokens(index, which):
        return normed.at[index % planes, block_of(which, half), :]

    mine = tokens(z, tp)

    @pl.when(z + 1 < planes)
    def _():
        remote(mine, mine, up_send.at[1], up_recv.at[1], above, tp).start()

    @pl.when(z > 0)
    def _():
        remote(mine, mine, down_send.at[1], down_recv.at[1], below, tp).start()

    remote(mine, mine, f_send.at[0], f_recv.at[0], sp, other).start()
    after = (p + 1) % plane
    zone = z + (p + 1) // plane

    @pl.when(jnp.logical_and(tp == 1, zone < planes))
    def _():
        for s in range(planes):
            for t in range(2):
                remote(
                    tail, halo.at[zone], h_send.at[s, t], h_recv.at[zone], s * plane + after, t
                ).start()

    share_weights(planes - 1, z == planes - 1, False)
    for d in range(planes - 2, 0, -1):
        share_weights(d)
        pass_weights(d + 1)
    for d in range(1, planes):

        @pl.when(z - d >= 0)
        def _():
            theirs = tokens(z + planes - d, tp)
            remote(theirs, theirs, up_send.at[d], up_recv.at[d], below, tp).wait_recv()

            @pl.when(z + 1 < planes)
            def _():
                remote(theirs, theirs, up_send.at[d + 1], up_recv.at[d + 1], above, tp).start()

            remote(theirs, theirs, f_send.at[d], f_recv.at[d], sp, other).start()

        @pl.when(z + d < planes)
        def _():
            theirs = tokens(z + d, tp)
            remote(theirs, theirs, down_send.at[d], down_recv.at[d], above, tp).wait_recv()

            @pl.when(z > 0)
            def _():
                remote(theirs, theirs, down_send.at[d + 1], down_recv.at[d + 1], below, tp).start()

            at = planes - d
            remote(theirs, theirs, f_send.at[at], f_recv.at[at], sp, other).start()

    for d in range(planes):
        theirs = tokens(z + planes - d, other)
        remote(theirs, theirs, f_send.at[d], f_recv.at[d], sp, other).wait()
    for s in range(planes):

        @pl.when(s * plane + p > 0)
        def _():
            remote(tail, halo.at[s], h_send.at[s, 0], h_recv.at[s], sp, other).wait_recv()

        @pl.when(s * plane + p == 0)
        def _():
            halo[s] = jnp.zeros(halo.shape[1:], halo.dtype)

    pass_weights(1)
    for copy in own_weights:
        copy.wait()
    for d in range(planes):
        for e in (3,) if square else ():
            there = partner(e)
            rows = block_of((z + planes - d) % planes * plane + there, tok)
            for m, dst in enumerate((lift_all, gate_all)):
                remote(
                    dst.at[rows, :], dst.at[rows, :], g_send.at[d, e, m], g_recv.at[d, e, m],
                    z * plane + there, tp,
                ).wait_recv()

    @pl.when(jnp.logical_and(tp == 1, zone < planes))
    def _():
        for s in range(planes):
            for t in range(2):
                remote(tail, halo.at[0], h_send.at[s, t], h_recv.at[0], sp, other).wait_send()

    for d in range(1, planes):

        @pl.when(jnp.logical_and(z + 1 < planes, z - d + 1 >= 0))
        def _():
            for e in range(plane):
                block = keys_of(z, e)
                remote(block, block, kv_send.at[d, e], kv_recv.at[d, e], above, tp).wait_send()
            remote(mine, mine, up_send.at[d], up_recv.at[d], above, tp).wait_send()

        @pl.when(jnp.logical_and(z > 0, z + d - 1 < planes))
        def _():
            remote(mine, mine, down_send.at[d], down_recv.at[d], below, tp).wait_send()

    for copy in started:
        copy.wait_send()


def down_kernel(
    plane, planes, starts, hidden, weight, stream, out,
    held, units, total, part, part_in, l_sem, own_sem, a_send, a_recv, t_send, t_recv,
):
    sp, tp = lax.axis_index("sp"), lax.axis_index("tp")
    z, p = sp // plane, sp % plane
    other = 1 - tp
    tok, width = units.shape[1:]
    half = tok // 2
    tiles = weight.shape[0] // 128

    def load(d):
        at = (z + planes - d) % planes
        first = pl.multiple_of(at * tiles // planes * 128, 128)
        return pltpu.make_async_copy(weight.at[pl.ds(first, width), :], held.at[d], l_sem.at[d])

    for d in range(planes):
        load(d).start()
    greet([((z + d) % planes * plane + p, tp) for d in range(1, planes)] + [(sp, other)])
    started = []
    own = pltpu.make_async_copy(hidden.at[z], units.at[z], own_sem)
    own.start()
    for d in range(1, planes):
        there = (z + d) % planes
        copy = remote(
            hidden.at[there], units.at[z], a_send.at[d], a_recv.at[d], there * plane + p, tp
        )
        copy.start()
        started.append(copy)
    columns = 512
    order = [0] + list(range(1, planes))
    for d in order:
        there = (z + planes - d) % planes
        load(d).wait()
        if d:
            remote(
                units.at[there], units.at[there], a_send.at[d], a_recv.at[d], sp, other
            ).wait_recv()
        else:
            own.wait()

        @pl.loop(0, weight.shape[1] // columns)
        def _(at):
            here = block_of(at, columns)
            term = jnp.dot(units[there], held[d, :, here], preferred_element_type=jnp.float32)
            total[:, here] = term if d == 0 else total[:, here] + term

    part[...] = total[block_of(other, half), :].astype(jnp.bfloat16)
    swap = remote(part, part_in, t_send, t_recv, sp, other)
    swap.start()
    started.append(swap)
    mine = total[block_of(tp, half), :].astype(jnp.bfloat16).astype(jnp.float32)
    swap.wait_recv()
    out[...] = (stream[...] + (mine + part_in[...].astype(jnp.float32))).astype(out.dtype)
    for copy in started:
        copy.wait_send()


def shorter_routes(
    plane, planes,
    query_one, key_one, query_two, key_two, values, mix_weight, head_gain, residual, out_weight,
    norm_gain, lift_weight, gate_weight, conv_taps, down_weight,
):
    bf16, f32 = jnp.bfloat16, jnp.float32
    tok = query_one.shape[0]
    model = residual.shape[1]
    val = 2 * HD
    ff = lift_weight.shape[1]
    tiles = ff // 128
    starts = [s * tiles // planes * 128 for s in range(planes + 1)]
    width = -(-tiles // planes) * 128
    count = planes * plane * tok
    sp = lax.axis_index("sp")
    z, p = sp // plane, sp % plane
    dma = pltpu.SemaphoreType.DMA
    anywhere = pl.BlockSpec(memory_space=pl.ANY)
    local = pl.BlockSpec(memory_space=pltpu.VMEM)
    shape = jax.ShapeDtypeStruct

    span = plane * tok
    pair = dma((planes + 1,))
    lift_all, gate_all, normed, halo, stream = pl.pallas_call(
        functools.partial(front_kernel, plane, planes, width),
        out_shape=(
            shape((count, width), bf16),
            shape((count, width), bf16),
            shape((planes, tok, model), bf16),
            shape((planes, 8, model), bf16),
            shape((tok // 2, model), f32),
        ),
        in_specs=[anywhere] * 7 + [pl.BlockSpec(memory_space=pltpu.SMEM)] + [local, anywhere, anywhere, local],
        out_specs=(anywhere, anywhere, local, local, local),
        scratch_shapes=[
            pltpu.VMEM((span, 2 * HD), bf16),
            pltpu.VMEM((count, 4 * HD), bf16),
            pltpu.VMEM((2, span, HD), f32),
            pltpu.VMEM((2, span, HD), f32),
            pltpu.VMEM((2, span, val), f32),
            pltpu.VMEM((span, val), bf16),
            pltpu.VMEM((plane, tok, val), bf16),
            pltpu.VMEM((tok // 2, model), bf16),
            pltpu.VMEM((tok // 2, model), bf16),
            pltpu.VMEM((8, model), bf16),
            pltpu.VMEM(out_weight.shape, bf16),
            pltpu.VMEM(residual.shape, bf16),
            dma((9,)), dma((plane, 5)), dma((plane, 5)), dma((planes, 2)), dma((planes, 2)),
            dma((planes + 1, plane)), dma((planes + 1, plane)), dma((planes, plane, 2)), dma((planes, plane, 2)),
            dma, dma((plane,)), dma((plane,)), dma, dma, pair, pair, pair, pair,
            dma((planes,)), dma((planes,)), dma((planes, 2)), dma((planes,)),
        ],
        compiler_params=pltpu.CompilerParams(
            collective_id=0, has_side_effects=True, vmem_limit_bytes=62 << 20
        ),
        name="front",
    )(
        query_one, key_one, query_two, key_two, values, lift_weight, gate_weight, mix_weight,
        head_gain.reshape(1, val), out_weight, residual, norm_gain.reshape(1, model),
    )

    rows = jnp.concatenate([halo, normed], axis=1).reshape(planes * (tok + 8), model)
    lifted = jnp.dot(rows, lift_all, preferred_element_type=f32).astype(bf16)
    gated = jnp.dot(rows, gate_all, preferred_element_type=f32).astype(bf16)
    lifted = lifted.reshape(planes, tok + 8, width)[:, 8:].astype(f32)
    gated = gated.reshape(planes, tok + 8, width).astype(f32)
    taps = lax.dynamic_slice_in_dim(conv_taps, z * tiles // planes * 128, width, 1)
    conv = 0.0
    for index in range(WIDTH):
        at = 8 - (WIDTH - 1) + index
        conv = conv + taps[index] * gated[:, at : at + tok]
    hidden = (jax.nn.silu(conv) * lifted).astype(bf16)
    mine = (z + 1) * tiles // planes * 128 - z * tiles // planes * 128
    hidden = jnp.where(lax.iota(jnp.int32, width) < mine, hidden, 0)

    return pl.pallas_call(
        functools.partial(down_kernel, plane, planes, starts),
        out_shape=shape((tok // 2, model), bf16),
        in_specs=[local, anywhere, local],
        out_specs=local,
        scratch_shapes=[
            pltpu.VMEM((planes, width, model), bf16),
            pltpu.VMEM((planes, tok, width), bf16),
            pltpu.VMEM((tok, model), f32),
            pltpu.VMEM((tok // 2, model), bf16),
            pltpu.VMEM((tok // 2, model), bf16),
            dma((planes,)), dma, dma((planes,)), dma((planes,)), dma, dma,
        ],
        compiler_params=pltpu.CompilerParams(
            collective_id=1, has_side_effects=True, vmem_limit_bytes=62 << 20
        ),
        name="down",
    )(hidden, down_weight, stream)


def any_route(*arrays):
    tok, heads, ff = arrays[0].shape[0], arrays[5].shape[0], arrays[10].shape[1]
    devices, groups = lax.axis_size("sp"), lax.axis_size("tp")
    planes = devices // heads
    fits = (
        groups == 2 and heads > 1 and planes > 1 and devices % heads == 0
        and ff % 128 == 0 and tok % 128 == 0 and WIDTH <= 9
        and arrays[10].shape[0] == tok
    )
    if fits:
        return shorter_routes(heads, planes, *arrays)
    return on_device(*arrays)


def solution(mesh):
    return jax.shard_map(
        any_route,
        mesh=mesh,
        in_specs=(
            P("sp", "tp"),
            P("sp", "tp"),
            P("sp", "tp"),
            P("sp", "tp"),
            P("sp", "tp"),
            P("tp"),
            P(),
            P(("sp", "tp"), None),
            P("tp", None),
            P(),
            P("sp", "tp"),
            P("sp", "tp"),
            P(None, "tp"),
            P("tp", None),
        ),
        out_specs=P(("sp", "tp"), None),
        check_vma=False,
    )
```

```python
import functools

import jax
import jax.numpy as jnp
from jax import lax
from jax.experimental import pallas as pl
from jax.experimental.pallas import tpu as pltpu
from jax.sharding import PartitionSpec as P

HD = 128
STRETCH = 64
WIDTH = 3


epsilon = 1e-06
masked_score = -1e30


def passed_along(block, axis, distance):
    devices = range(lax.axis_size(axis))
    route = [(i - distance, i) for i in devices if i - distance in devices]
    return lax.ppermute(block, axis, route)


def update_map(peak, total, acc, queries, keys, vals, visible):
    scores = jnp.einsum("thd,shd->hts", queries, keys, preferred_element_type=jnp.float32) * HD ** (
        -0.5
    )
    scores = jnp.where(visible[None], scores, masked_score)
    new_peak = jnp.maximum(peak, jnp.max(scores, axis=-1))
    weights = jnp.where(visible[None], jnp.exp(scores - new_peak[..., None]), 0.0)
    total = jnp.sum(weights, axis=-1)
    acc = jnp.einsum(
        "hts,she->hte", weights.astype(jnp.bfloat16), vals, preferred_element_type=jnp.float32
    )
    return (new_peak, total, acc)


def on_device(
    query_one,
    key_one,
    query_two,
    key_two,
    values,
    mix_weight,
    head_gain,
    residual,
    out_weight,
    norm_gain,
    lift_weight,
    gate_weight,
    conv_taps,
    down_weight,
):
    tok_local = query_one.shape[0]
    heads_local = mix_weight.shape[0]
    val_width = values.shape[1] // heads_local
    model_width = residual.shape[1]
    offset = lax.axis_index("sp") * tok_local
    q_pos = offset + lax.iota(jnp.int32, tok_local)
    q_one = query_one.reshape(tok_local, heads_local, HD)
    q_two = query_two.reshape(tok_local, heads_local, HD)
    start_peak = jnp.full((heads_local, tok_local), masked_score, jnp.float32)
    start_total = jnp.zeros((heads_local, tok_local), jnp.float32)
    start_acc = jnp.zeros((heads_local, tok_local, val_width), jnp.float32)
    initial = (start_peak, start_total, start_acc, start_peak, start_total, start_acc)
    first_keys = lax.all_gather(key_one, "sp", axis=0, tiled=True)
    second_keys = lax.all_gather(key_two, "sp", axis=0, tiled=True)
    piece_vals = lax.all_gather(values, "sp", axis=0, tiled=True)
    count = first_keys.shape[0]
    k_pos = lax.iota(jnp.int32, count)
    visible = k_pos[None, :] // STRETCH <= q_pos[:, None] // STRETCH
    first_keys = first_keys.reshape(count, heads_local, HD)
    second_keys = second_keys.reshape(count, heads_local, HD)
    piece_vals = piece_vals.reshape(count, heads_local, val_width)
    first = update_map(initial[0], initial[1], initial[2], q_one, first_keys, piece_vals, visible)
    second = update_map(initial[3], initial[4], initial[5], q_two, second_keys, piece_vals, visible)
    state = first + second
    mixed = (
        state[2] / state[1][..., None] - mix_weight[:, None, None] * state[5] / state[4][..., None]
    )
    head_out = (
        mixed * lax.rsqrt(jnp.mean(mixed * mixed, axis=-1, keepdims=True) + epsilon) * head_gain
    ).astype(jnp.bfloat16)
    out_heads = out_weight.reshape(heads_local, val_width, model_width)
    piece = head_out
    attended = lax.psum_scatter(
        jnp.einsum("hte,hed->td", piece, out_heads, preferred_element_type=jnp.float32).astype(
            jnp.bfloat16
        ),
        "tp",
        scatter_dimension=0,
        tiled=True,
    ).astype(jnp.float32)
    stream = residual.astype(jnp.float32) + attended
    normed = (
        stream * lax.rsqrt(jnp.mean(stream * stream, axis=-1, keepdims=True) + epsilon) * norm_gain
    ).astype(jnp.bfloat16)
    whole_rows = lax.all_gather(normed, "tp", axis=0, tiled=True)
    lift_pre = jnp.dot(
        whole_rows,
        lax.all_gather(lift_weight, "sp", axis=0, tiled=True),
        preferred_element_type=jnp.float32,
    )
    gate_pre = jnp.dot(
        whole_rows,
        lax.all_gather(gate_weight, "sp", axis=0, tiled=True),
        preferred_element_type=jnp.float32,
    )
    lifted = lift_pre.astype(jnp.bfloat16)
    gated = gate_pre.astype(jnp.bfloat16)
    prior = passed_along(gated[tok_local - (WIDTH - 1) :], "sp", 1)
    extended = jnp.concatenate([prior, gated], axis=0).astype(jnp.float32)
    conv = conv_taps[0] * extended[0:tok_local]
    for index in range(1, WIDTH):
        conv = conv + conv_taps[index] * extended[index : index + tok_local]
    hidden = (jax.nn.silu(conv) * lifted.astype(jnp.float32)).astype(jnp.bfloat16)
    piece = hidden
    mixer = lax.psum_scatter(
        jnp.dot(piece, down_weight, preferred_element_type=jnp.float32).astype(jnp.bfloat16),
        "tp",
        scatter_dimension=0,
        tiled=True,
    ).astype(jnp.float32)
    return (stream + mixer).astype(jnp.bfloat16)

MESH = pl.DeviceIdType.MESH


def remote(src, dst, send_sem, recv_sem, sp, tp):
    return pltpu.make_async_remote_copy(
        src_ref=src,
        dst_ref=dst,
        send_sem=send_sem,
        recv_sem=recv_sem,
        device_id=(sp, tp),
        device_id_type=MESH,
    )


def greet(peers, count=None):
    barrier = pltpu.get_barrier_semaphore()
    for peer in peers:
        pl.semaphore_signal(barrier, inc=1, device_id=peer, device_id_type=MESH)
    pl.semaphore_wait(barrier, len(peers) if count is None else count)


def block_of(index, size):
    return pl.ds(pl.multiple_of(index * size, size), size)


def front_kernel(
    plane, planes, width, q1, k1, q2, k2, v, lift, gate, mix_weight, head_gain, out_hbm, residual_hbm,
    gain,
    lift_all, gate_all, normed, halo, stream,
    q_all, kv_all, peaks, totals, sums, head_out, heads, part, part_in, tail, out_weight, residual,
    own_sem, a_send, a_recv, w_send, w_recv, kv_send, kv_recv, g_send, g_recv,
    b_own, b_send, b_recv, t_send, t_recv, up_send, up_recv, down_send, down_recv,
    f_send, f_recv, h_send, h_recv,
):
    sp, tp = lax.axis_index("sp"), lax.axis_index("tp")
    z, p = sp // plane, sp % plane
    other = 1 - tp
    tok = q1.shape[0]
    half = tok // 2
    val = 2 * HD
    tiles = lift.shape[1] // 128
    before = (p + plane - 1) % plane
    above, below = (z + 1) % planes * plane + p, (z + planes - 1) % planes * plane + p
    weights = ((lift, lift_all), (gate, gate_all))
    peers = (
        [(z * plane + (p + d) % plane, tp) for d in range(1, plane)]
        + [((z + d) % planes * plane + p, tp) for d in range(1, planes)]
        + [(sp, other)]
    )
    barrier = pltpu.get_barrier_semaphore()
    for peer in peers + [(s * plane + before, 1) for s in range(planes)]:
        pl.semaphore_signal(barrier, inc=1, device_id=peer, device_id_type=MESH)

    def piece(head, row):
        h1, h2 = block_of(head, HD), block_of(head, 2 * HD)
        rows, all_rows = block_of(row % plane, tok), block_of(row, tok)
        return [
            (k1.at[:, h1], kv_all.at[all_rows, 0:HD]),
            (k2.at[:, h1], kv_all.at[all_rows, HD : 2 * HD]),
            (v.at[:, h2], kv_all.at[all_rows, 2 * HD : 4 * HD]),
            (q1.at[:, h1], q_all.at[rows, 0:HD]),
            (q2.at[:, h1], q_all.at[rows, HD : 2 * HD]),
        ]

    def units(index):
        return pl.ds(pl.multiple_of(index * tiles // planes * 128, 128), width)

    started = []
    own = [
        pltpu.make_async_copy(src, dst, own_sem.at[n]) for n, (src, dst) in enumerate(piece(p, sp))
    ]
    own_weights = [
        pltpu.make_async_copy(src.at[:, units(z)], dst.at[block_of(sp, tok), :], own_sem.at[5 + m])
        for m, (src, dst) in enumerate(weights)
    ]
    for copy in own:
        copy.start()
    loads = [
        pltpu.make_async_copy(out_hbm, out_weight, own_sem.at[7]),
        pltpu.make_async_copy(residual_hbm, residual, own_sem.at[8]),
    ]
    pl.semaphore_wait(barrier, len(peers) + 2 * planes * tp)
    for part_of in ((0, 1, 2), (3, 4)):
        for d in range(1, plane):
            there = (p + d) % plane
            pairs = piece(there, sp)
            for n in part_of:
                src, dst = pairs[n]
                copy = remote(src, dst, a_send.at[d, n], a_recv.at[d, n], z * plane + there, tp)
                copy.start()
                started.append(copy)

    lanes = {}
    for d in range(1, planes):
        there = (z + d) % planes
        lanes[d] = [
            remote(
                src.at[:, units(there)], dst.at[block_of(sp, tok), :],
                w_send.at[d, m], w_recv.at[d, m], there * plane + p, tp,
            )
            for m, (src, dst) in enumerate(weights)
        ]
        started.extend(lanes[d])

    def send_weights(early):
        for d in range(planes - 1, 0, -1):

            if d == planes - 1:
                turn = (z > 0) if early else None
            else:
                turn = (z + d >= planes) if early else (z + d < planes)
            if turn is None:
                continue

            @pl.when(turn)
            def _():
                for copy in lanes[d]:
                    copy.start()

    square = plane == 4
    direct = (1, 2) if square else range(1, plane)

    def partner(e):
        if not square:
            return (p + e) % plane
        flips = {1: p + 1 - 2 * (p % 2), 2: (p + 2) % 4, 3: 3 - p}
        return flips[e]

    def share_weights(d):
        source = (z + planes - d) % planes * plane + p
        rows = block_of(source, tok)
        for m, dst in enumerate((lift_all, gate_all)):
            if d:
                remote(
                    dst.at[rows, :], dst.at[rows, :], w_send.at[d, m], w_recv.at[d, m], source, tp
                ).wait_recv()
            src = dst.at[rows, :] if d else weights[m][0].at[:, units(z)]
            for e in direct:
                copy = remote(
                    src, dst.at[rows, :], g_send.at[d, e, m], g_recv.at[d, e, m],
                    z * plane + partner(e), tp,
                )
                copy.start()
                started.append(copy)

    def pass_weights(d):
        for m, dst in enumerate((lift_all, gate_all)):
            for e in direct:
                there = partner(e) if square else (p + plane - e) % plane
                rows = block_of((z + planes - d) % planes * plane + there, tok)
                block = dst.at[rows, :]
                remote(
                    block, block, g_send.at[d, e, m], g_recv.at[d, e, m], z * plane + there, tp
                ).wait_recv()
                if square and e == m + 1:
                    copy = remote(
                        block, block, g_send.at[d, 3, m], g_recv.at[d, 3, m],
                        z * plane + partner(3 - e), tp,
                    )
                    copy.start()
                    started.append(copy)

    send_weights(True)
    share_weights(0)
    for copy in own_weights + loads:
        copy.start()
    span = plane * tok

    def keys_of(index, e):
        return kv_all.at[block_of(index * plane + (p + plane - e) % plane, tok), :]

    def arrival(e, which):
        source = z * plane + (p + plane - e) % plane
        pairs = piece(p, source)
        for n in which:
            src, dst = pairs[n]
            remote(src, dst, a_send.at[e, n], a_recv.at[e, n], source, tp).wait_recv()

    for e in range(plane):
        if e:
            arrival(e, (0, 1, 2))
        else:
            for copy in own[:3]:
                copy.wait()

        @pl.when(z + 1 < planes)
        def _():
            block = keys_of(z, e)
            remote(block, block, kv_send.at[1, e], kv_recv.at[1, e], above, tp).start()

    @pl.when(z == 0)
    def _():
        for copy in lanes[planes - 1]:
            copy.start()

    for copy in own[3:]:
        copy.wait()
    for e in range(1, plane):
        arrival(e, (3, 4))

    def attend(source, first):
        @pl.loop(0, plane)
        def _(chunk):
            rows, keys = block_of(chunk, tok), block_of(source, span)
            for m in range(2):
                scores = lax.dot_general(
                    q_all[rows, m * HD : (m + 1) * HD],
                    kv_all[keys, m * HD : (m + 1) * HD],
                    (((1,), (1,)), ((), ())),
                    preferred_element_type=jnp.float32,
                ) * HD ** (-0.5)
                if first:
                    k_pos = lax.broadcasted_iota(jnp.int32, (tok, span), 1)
                    q_pos = chunk * tok + lax.broadcasted_iota(jnp.int32, (tok, span), 0)
                    visible = lax.div(k_pos, STRETCH) <= lax.div(q_pos, STRETCH)
                    scores = jnp.where(visible, scores, masked_score)
                    peak = jnp.max(scores, axis=-1, keepdims=True)
                    terms = jnp.where(visible, jnp.exp(scores - peak), 0.0)
                else:
                    last = peaks[m, rows, 0:1]
                    peak = jnp.maximum(last, jnp.max(scores, axis=-1, keepdims=True))
                    terms = jnp.exp(scores - peak)
                total = jnp.sum(terms, axis=-1, keepdims=True)
                acc = jnp.dot(
                    terms.astype(jnp.bfloat16),
                    kv_all[keys, 2 * HD : 4 * HD],
                    preferred_element_type=jnp.float32,
                )
                if not first:
                    fade = jnp.exp(last - peak)
                    total = total + fade * totals[m, rows, 0:1]
                    acc = acc + fade * sums[m, rows, :]
                peaks[m, rows, :] = jnp.broadcast_to(peak, (tok, HD))
                totals[m, rows, :] = jnp.broadcast_to(total, (tok, HD))
                sums[m, rows, :] = acc

    attend(z, True)
    for d in range(1, planes):

        @pl.when(z - d >= 0)
        def _():
            for e in range(plane):
                here = keys_of((z + planes - d) % planes, e)
                remote(here, here, kv_send.at[d, e], kv_recv.at[d, e], below, tp).wait_recv()

                @pl.when(z + 1 < planes)
                def _():
                    remote(
                        here, here, kv_send.at[d + 1, e], kv_recv.at[d + 1, e], above, tp
                    ).start()

        @pl.when(z - d >= 0)
        def _():
            attend((z + planes - d) % planes, False)

        if d == 1:
            pass_weights(0)

    send_weights(False)

    @pl.loop(0, plane)
    def _(chunk):
        rows = block_of(chunk, tok)
        mixed = (
            sums[0, rows, :] / totals[0, rows, 0:1]
            - mix_weight[p] * sums[1, rows, :] / totals[1, rows, 0:1]
        )
        scale = lax.rsqrt(jnp.mean(mixed * mixed, axis=-1, keepdims=True) + epsilon)
        head_out[rows, :] = (mixed * scale * head_gain[...]).astype(jnp.bfloat16)

    own = pltpu.make_async_copy(head_out.at[block_of(p, tok), :], heads.at[p], b_own)
    own.start()
    for d in range(1, plane):
        there = (p + d) % plane
        copy = remote(
            head_out.at[block_of(there, tok), :], heads.at[p],
            b_send.at[d], b_recv.at[d], z * plane + there, tp,
        )
        copy.start()
        started.append(copy)
    own.wait()
    share_weights(planes - 1)
    for d in range(1, plane):
        there = (p + plane - d) % plane
        remote(
            heads.at[there], heads.at[there], b_send.at[d], b_recv.at[d], z * plane + there, tp
        ).wait_recv()

    for copy in loads:
        copy.wait()
    columns = 512

    def product(which, at):
        total = None
        for h in range(plane):
            term = jnp.dot(
                heads[h, block_of(which, half), :],
                out_weight[h * val : (h + 1) * val, at : at + columns],
                preferred_element_type=jnp.float32,
            )
            total = term if total is None else total + term
        return total.astype(jnp.bfloat16)

    model = out_weight.shape[1]
    for at in range(0, model, columns):
        part[:, at : at + columns] = product(other, at)
    swap = remote(part, part_in, t_send, t_recv, sp, other)
    swap.start()
    started.append(swap)
    for at in range(0, model, columns):
        stream[:, at : at + columns] = product(tp, at).astype(jnp.float32)
    swap.wait_recv()
    whole = residual[...].astype(jnp.float32) + (stream[...] + part_in[...].astype(jnp.float32))
    stream[...] = whole
    scaled = whole * lax.rsqrt(jnp.mean(whole * whole, axis=-1, keepdims=True) + epsilon) * gain[...]
    normed[z, block_of(tp, half), :] = scaled.astype(jnp.bfloat16)
    tail[...] = scaled[half - 8 :, :].astype(jnp.bfloat16)

    def tokens(index, which):
        return normed.at[index % planes, block_of(which, half), :]

    mine = tokens(z, tp)

    @pl.when(z + 1 < planes)
    def _():
        remote(mine, mine, up_send.at[1], up_recv.at[1], above, tp).start()

    @pl.when(z > 0)
    def _():
        remote(mine, mine, down_send.at[1], down_recv.at[1], below, tp).start()

    remote(mine, mine, f_send.at[0], f_recv.at[0], sp, other).start()
    after = (p + 1) % plane
    zone = z + (p + 1) // plane

    @pl.when(jnp.logical_and(tp == 1, zone < planes))
    def _():
        for s in range(planes):
            for t in range(2):
                remote(
                    tail, halo.at[zone], h_send.at[s, t], h_recv.at[zone], s * plane + after, t
                ).start()

    for d in range(planes - 2, 0, -1):
        share_weights(d)
        pass_weights(d + 1)
    for d in range(1, planes):

        @pl.when(z - d >= 0)
        def _():
            theirs = tokens(z + planes - d, tp)
            remote(theirs, theirs, up_send.at[d], up_recv.at[d], below, tp).wait_recv()

            @pl.when(z + 1 < planes)
            def _():
                remote(theirs, theirs, up_send.at[d + 1], up_recv.at[d + 1], above, tp).start()

            remote(theirs, theirs, f_send.at[d], f_recv.at[d], sp, other).start()

        @pl.when(z + d < planes)
        def _():
            theirs = tokens(z + d, tp)
            remote(theirs, theirs, down_send.at[d], down_recv.at[d], above, tp).wait_recv()

            @pl.when(z > 0)
            def _():
                remote(theirs, theirs, down_send.at[d + 1], down_recv.at[d + 1], below, tp).start()

            at = planes - d
            remote(theirs, theirs, f_send.at[at], f_recv.at[at], sp, other).start()

    for d in range(planes):
        theirs = tokens(z + planes - d, other)
        remote(theirs, theirs, f_send.at[d], f_recv.at[d], sp, other).wait()
    for s in range(planes):

        @pl.when(s * plane + p > 0)
        def _():
            remote(tail, halo.at[s], h_send.at[s, 0], h_recv.at[s], sp, other).wait_recv()

        @pl.when(s * plane + p == 0)
        def _():
            halo[s] = jnp.zeros(halo.shape[1:], halo.dtype)

    pass_weights(1)
    for copy in own_weights:
        copy.wait()
    for d in range(planes):
        for e in (3,) if square else ():
            there = partner(e)
            rows = block_of((z + planes - d) % planes * plane + there, tok)
            for m, dst in enumerate((lift_all, gate_all)):
                remote(
                    dst.at[rows, :], dst.at[rows, :], g_send.at[d, e, m], g_recv.at[d, e, m],
                    z * plane + there, tp,
                ).wait_recv()

    @pl.when(jnp.logical_and(tp == 1, zone < planes))
    def _():
        for s in range(planes):
            for t in range(2):
                remote(tail, halo.at[0], h_send.at[s, t], h_recv.at[0], sp, other).wait_send()

    for d in range(1, planes):

        @pl.when(jnp.logical_and(z + 1 < planes, z - d + 1 >= 0))
        def _():
            for e in range(plane):
                block = keys_of(z, e)
                remote(block, block, kv_send.at[d, e], kv_recv.at[d, e], above, tp).wait_send()
            remote(mine, mine, up_send.at[d], up_recv.at[d], above, tp).wait_send()

        @pl.when(jnp.logical_and(z > 0, z + d - 1 < planes))
        def _():
            remote(mine, mine, down_send.at[d], down_recv.at[d], below, tp).wait_send()

    for copy in started:
        copy.wait_send()


def down_kernel(
    plane, planes, starts, hidden, weight, stream, out,
    held, units, total, part, part_in, l_sem, own_sem, a_send, a_recv, t_send, t_recv,
):
    sp, tp = lax.axis_index("sp"), lax.axis_index("tp")
    z, p = sp // plane, sp % plane
    other = 1 - tp
    tok, width = units.shape[1:]
    half = tok // 2
    tiles = weight.shape[0] // 128

    def load(d):
        at = (z + planes - d) % planes
        first = pl.multiple_of(at * tiles // planes * 128, 128)
        return pltpu.make_async_copy(weight.at[pl.ds(first, width), :], held.at[d], l_sem.at[d])

    for d in range(planes):
        load(d).start()
    greet([((z + d) % planes * plane + p, tp) for d in range(1, planes)] + [(sp, other)])
    started = []
    own = pltpu.make_async_copy(hidden.at[z], units.at[z], own_sem)
    own.start()
    for d in range(1, planes):
        there = (z + d) % planes
        copy = remote(
            hidden.at[there], units.at[z], a_send.at[d], a_recv.at[d], there * plane + p, tp
        )
        copy.start()
        started.append(copy)
    columns = 512
    order = [0] + list(range(1, planes))
    for d in order:
        there = (z + planes - d) % planes
        load(d).wait()
        if d:
            remote(
                units.at[there], units.at[there], a_send.at[d], a_recv.at[d], sp, other
            ).wait_recv()
        else:
            own.wait()

        @pl.loop(0, weight.shape[1] // columns)
        def _(at):
            here = block_of(at, columns)
            term = jnp.dot(units[there], held[d, :, here], preferred_element_type=jnp.float32)
            total[:, here] = term if d == 0 else total[:, here] + term

    part[...] = total[block_of(other, half), :].astype(jnp.bfloat16)
    swap = remote(part, part_in, t_send, t_recv, sp, other)
    swap.start()
    started.append(swap)
    mine = total[block_of(tp, half), :].astype(jnp.bfloat16).astype(jnp.float32)
    swap.wait_recv()
    out[...] = (stream[...] + (mine + part_in[...].astype(jnp.float32))).astype(out.dtype)
    for copy in started:
        copy.wait_send()


def shorter_routes(
    plane, planes,
    query_one, key_one, query_two, key_two, values, mix_weight, head_gain, residual, out_weight,
    norm_gain, lift_weight, gate_weight, conv_taps, down_weight,
):
    bf16, f32 = jnp.bfloat16, jnp.float32
    tok = query_one.shape[0]
    model = residual.shape[1]
    val = 2 * HD
    ff = lift_weight.shape[1]
    tiles = ff // 128
    starts = [s * tiles // planes * 128 for s in range(planes + 1)]
    width = -(-tiles // planes) * 128
    count = planes * plane * tok
    sp = lax.axis_index("sp")
    z, p = sp // plane, sp % plane
    dma = pltpu.SemaphoreType.DMA
    anywhere = pl.BlockSpec(memory_space=pl.ANY)
    local = pl.BlockSpec(memory_space=pltpu.VMEM)
    shape = jax.ShapeDtypeStruct

    span = plane * tok
    pair = dma((planes + 1,))
    lift_all, gate_all, normed, halo, stream = pl.pallas_call(
        functools.partial(front_kernel, plane, planes, width),
        out_shape=(
            shape((count, width), bf16),
            shape((count, width), bf16),
            shape((planes, tok, model), bf16),
            shape((planes, 8, model), bf16),
            shape((tok // 2, model), f32),
        ),
        in_specs=[anywhere] * 7 + [pl.BlockSpec(memory_space=pltpu.SMEM)] + [local, anywhere, anywhere, local],
        out_specs=(anywhere, anywhere, local, local, local),
        scratch_shapes=[
            pltpu.VMEM((span, 2 * HD), bf16),
            pltpu.VMEM((count, 4 * HD), bf16),
            pltpu.VMEM((2, span, HD), f32),
            pltpu.VMEM((2, span, HD), f32),
            pltpu.VMEM((2, span, val), f32),
            pltpu.VMEM((span, val), bf16),
            pltpu.VMEM((plane, tok, val), bf16),
            pltpu.VMEM((tok // 2, model), bf16),
            pltpu.VMEM((tok // 2, model), bf16),
            pltpu.VMEM((8, model), bf16),
            pltpu.VMEM(out_weight.shape, bf16),
            pltpu.VMEM(residual.shape, bf16),
            dma((9,)), dma((plane, 5)), dma((plane, 5)), dma((planes, 2)), dma((planes, 2)),
            dma((planes + 1, plane)), dma((planes + 1, plane)), dma((planes, plane, 2)), dma((planes, plane, 2)),
            dma, dma((plane,)), dma((plane,)), dma, dma, pair, pair, pair, pair,
            dma((planes,)), dma((planes,)), dma((planes, 2)), dma((planes,)),
        ],
        compiler_params=pltpu.CompilerParams(
            collective_id=0, has_side_effects=True, vmem_limit_bytes=62 << 20
        ),
        name="front",
    )(
        query_one, key_one, query_two, key_two, values, lift_weight, gate_weight, mix_weight,
        head_gain.reshape(1, val), out_weight, residual, norm_gain.reshape(1, model),
    )

    rows = jnp.concatenate([halo, normed], axis=1).reshape(planes * (tok + 8), model)
    lifted = jnp.dot(rows, lift_all, preferred_element_type=f32).astype(bf16)
    gated = jnp.dot(rows, gate_all, preferred_element_type=f32).astype(bf16)
    lifted = lifted.reshape(planes, tok + 8, width)[:, 8:].astype(f32)
    gated = gated.reshape(planes, tok + 8, width).astype(f32)
    taps = lax.dynamic_slice_in_dim(conv_taps, z * tiles // planes * 128, width, 1)
    conv = 0.0
    for index in range(WIDTH):
        at = 8 - (WIDTH - 1) + index
        conv = conv + taps[index] * gated[:, at : at + tok]
    hidden = (jax.nn.silu(conv) * lifted).astype(bf16)
    mine = (z + 1) * tiles // planes * 128 - z * tiles // planes * 128
    hidden = jnp.where(lax.iota(jnp.int32, width) < mine, hidden, 0)

    return pl.pallas_call(
        functools.partial(down_kernel, plane, planes, starts),
        out_shape=shape((tok // 2, model), bf16),
        in_specs=[local, anywhere, local],
        out_specs=local,
        scratch_shapes=[
            pltpu.VMEM((planes, width, model), bf16),
            pltpu.VMEM((planes, tok, width), bf16),
            pltpu.VMEM((tok, model), f32),
            pltpu.VMEM((tok // 2, model), bf16),
            pltpu.VMEM((tok // 2, model), bf16),
            dma((planes,)), dma, dma((planes,)), dma((planes,)), dma, dma,
        ],
        compiler_params=pltpu.CompilerParams(
            collective_id=1, has_side_effects=True, vmem_limit_bytes=62 << 20
        ),
        name="down",
    )(hidden, down_weight, stream)


def any_route(*arrays):
    tok, heads, ff = arrays[0].shape[0], arrays[5].shape[0], arrays[10].shape[1]
    devices, groups = lax.axis_size("sp"), lax.axis_size("tp")
    planes = devices // heads
    fits = (
        groups == 2 and heads > 1 and planes > 1 and devices % heads == 0
        and ff % 128 == 0 and tok % 128 == 0 and WIDTH <= 9
        and arrays[10].shape[0] == tok
    )
    if fits:
        return shorter_routes(heads, planes, *arrays)
    return on_device(*arrays)


def solution(mesh):
    return jax.shard_map(
        any_route,
        mesh=mesh,
        in_specs=(
            P("sp", "tp"),
            P("sp", "tp"),
            P("sp", "tp"),
            P("sp", "tp"),
            P("sp", "tp"),
            P("tp"),
            P(),
            P(("sp", "tp"), None),
            P("tp", None),
            P(),
            P("sp", "tp"),
            P("sp", "tp"),
            P(None, "tp"),
            P("tp", None),
        ),
        out_specs=P(("sp", "tp"), None),
        check_vma=False,
    )
```
